128 devices in a mesh: kv: 32 (over z, y, core), tp: 4 (over x).
Axes of the slice: x: 4, y: 4, z: 4, core: 2. Of those that a mesh axis runs over, the one named last changes fastest.
Arguments:
- tokens: bfloat16 [512, 4, 4096], P('kv'), may hold values from -6 to 6
- norm_gain: bfloat16 [4096], replicated, may hold values from 0.099609375 to 1.8984375
- query_weight: bfloat16 [4096, 2048], P(None, 'tp'), may hold values from -0.09375 to 0.09375
- key_weight: bfloat16 [4096, 2048], P(None, 'tp'), may hold values from -0.09375 to 0.09375
- value_weight: bfloat16 [4096, 2048], P(None, 'tp'), may hold values from -0.09375 to 0.09375
- outgate_weight: bfloat16 [4096, 2048], P(None, 'tp'), may hold values from -0.09375 to 0.09375
- gate_weight: bfloat16 [4096, 32], replicated, may hold values from -0.09375 to 0.09375
- gate_bias: float32 [2, 16], replicated, may hold values from -1 to 4
- head_gain: bfloat16 [2048], P('tp'), may hold values from 0.099609375 to 1.8984375
- out_weight: bfloat16 [2048, 4096], P('tp', 'kv'), may hold values from -0.125 to 0.125
- state_c: float32 [512, 16, 128, 128], P('kv', 'tp'), may hold values from -3 to 3
- state_n: float32 [512, 16, 128], P('kv', 'tp'), may hold values from -3 to 3
- state_m: float32 [512, 16], P('kv', 'tp'), may hold values from -1 to 2
- prev_keys: bfloat16 [512, 16, 4, 128], P('kv', 'tp'), may hold values from -6 to 6
- prev_values: bfloat16 [512, 16, 4, 128], P('kv', 'tp'), may hold values from -6 to 6
- prev_gates: float32 [512, 16, 2, 4], P('kv', 'tp'), may hold values from -2 to 5
- accepted: int32 [512], P('kv'), may hold values from 0 to 4
Outputs:
- mixed: bfloat16 [512, 4, 4096], P(None, None, 'kv')
- carried_c: float32 [512, 16, 128, 128], P('kv', 'tp')
- carried_n: float32 [512, 16, 128], P('kv', 'tp')
- carried_m: float32 [512, 16], P('kv', 'tp')
- step_keys: bfloat16 [512, 16, 4, 128], P('kv', 'tp')
- step_values: bfloat16 [512, 16, 4, 128], P('kv', 'tp')
- step_gates: float32 [512, 16, 2, 4], P('kv', 'tp')
The draws below stay inside these ranges and needn't reach their ends.
Inputs may be any that keep to these rules, and one draw needn't show every extreme that they name: accepted counts proposals of the last step, from none to all 4.
All inputs are finite; a program needn't handle non-finite values.
Results may differ from the reference program's by a relative error of at most 0.0075.
The reference program's roundings to bfloat16 on the way (of `normed`, `queries`, `outgate` and `gated`) count: a program that leaves them out, or rounds other values in their place, can miss the bound.
Values may be sent and summed in bfloat16 or wider, within the bound.
No kernel may reach another device: no remote copies, remote signals or barrier semaphores. Data moves between devices by JAX's collectives and lax.ppermute only.
A program may use at most 128 MiB of HBM per device.

```python
import jax
import jax.numpy as jnp
from jax import lax

D = 4096
HEADS = 16
DH = 128
PROPS = 4
BATCH = 512
MIX = 2048


def touch_ends(values, rng, smallest, top_value):
    spot = [jax.random.randint(jax.random.fold_in(rng, axis), (), 0, length) for axis, length in enumerate(values.shape)]
    main_axis = values.shape.index(max(values.shape))
    neighbour = spot[:main_axis] + [(spot[main_axis] + 1) % values.shape[main_axis]] + spot[main_axis + 1:]
    return values.at[tuple(spot)].set(smallest).at[tuple(neighbour)].set(top_value)


def level_of(stream_key, dims, split, low, largest):
    loudness, own = 1.0, jax.random.fold_in(stream_key, 6)
    for axis_at, parts in split:
        draws = jnp.exp(jax.random.uniform(jax.random.fold_in(own, axis_at), (parts,), jnp.float32, low / len(split), largest / len(split)))
        loudness = loudness * jnp.repeat(draws, dims[axis_at] // parts).reshape([-1 if axis == axis_at else 1 for axis in range(len(dims))])
    return loudness


def normal_values(rng, extent, width, most, pieces=(), kind=jnp.bfloat16):
    values = jax.random.normal(rng, extent, jnp.float32) * width
    if len(pieces) > 0:
        values = level_of(rng, extent, pieces, -0.22, 0.18) * values
    return jnp.clip(values, min=-most, max=most).astype(kind)


def setup_inputs(seed: int = 0) -> dict:
    streams_of = jax.random.split(jax.random.key(seed), 18)
    tokens = normal_values(streams_of[0], (BATCH, PROPS, D), 1.0, 6.0, ((0, 32),))
    norm_gain = jnp.clip(1.0 + 0.18 * jax.random.normal(streams_of[1], (D,), jnp.float32), 0.099609375, 1.8984375).astype(jnp.bfloat16)
    query_weight = normal_values(streams_of[2], (D, MIX), D ** -0.5, 0.09375, ((1, 4),))
    key_weight = normal_values(streams_of[3], (D, MIX), D ** -0.5, 0.09375, ((1, 4),))
    value_weight = normal_values(streams_of[4], (D, MIX), D ** -0.5, 0.09375, ((1, 4),))
    outgate_weight = normal_values(streams_of[5], (D, MIX), D ** -0.5, 0.09375, ((1, 4),))
    gate_weight = normal_values(streams_of[6], (D, 2 * HEADS), D ** -0.5, 0.09375)
    gate_bias = jnp.clip(jax.random.uniform(streams_of[7], (2, HEADS), jnp.float32, -1.0, 4.0), -1.0, 4.0)
    head_gain = jnp.clip(1.0 + 0.18 * jax.random.normal(streams_of[8], (MIX,), jnp.float32), 0.099609375, 1.8984375).astype(jnp.bfloat16)
    out_weight = normal_values(streams_of[9], (MIX, D), MIX ** -0.5, 0.125, ((0, 4), (1, 32)))
    state_c = normal_values(streams_of[10], (BATCH, HEADS, DH, DH), 0.3, 3.0, ((0, 32), (1, 4)), jnp.float32)
    state_n = normal_values(streams_of[11], (BATCH, HEADS, DH), 0.3, 3.0, ((0, 32), (1, 4)), jnp.float32)
    state_m = jnp.clip(-1.0 + 3.0 * jax.random.uniform(streams_of[12], (BATCH, HEADS), jnp.float32) ** level_of(streams_of[12], (BATCH, HEADS), ((0, 32), (1, 4)), -0.2, 0.2), -1.0, 2.0)
    prev_keys = normal_values(streams_of[13], (BATCH, HEADS, PROPS, DH), 1.0, 6.0, ((0, 32), (1, 4)))
    prev_values = normal_values(streams_of[14], (BATCH, HEADS, PROPS, DH), 1.0, 6.0, ((0, 32), (1, 4)))
    prev_gates = jnp.clip(-2.0 + 7.0 * jax.random.uniform(streams_of[15], (BATCH, HEADS, 2, PROPS), jnp.float32) ** level_of(streams_of[15], (BATCH, HEADS, 2, PROPS), ((0, 32), (1, 4)), -0.2, 0.2), -2.0, 5.0)
    accepted = touch_ends(jax.random.randint(streams_of[16], (BATCH,), 0, PROPS + 1), jax.random.fold_in(streams_of[16], 1), 0, PROPS).astype(jnp.int32)
    return {"tokens": tokens, "norm_gain": norm_gain, "query_weight": query_weight, "key_weight": key_weight, "value_weight": value_weight, "outgate_weight": outgate_weight, "gate_weight": gate_weight, "gate_bias": gate_bias, "head_gain": head_gain, "out_weight": out_weight, "state_c": state_c, "state_n": state_n, "state_m": state_m, "prev_keys": prev_keys, "prev_values": prev_values, "prev_gates": prev_gates, "accepted": accepted}


EPSILON = 1e-06
HIGHEST = lax.Precision.HIGHEST

def replay(state_c, state_n, state_m, keys_in, values_in, gates_in, accepted):
    proposals = keys_in.shape[2]
    scaled = keys_in.astype(jnp.float32) * keys_in.shape[3] ** (-0.5)
    values_f = values_in.astype(jnp.float32)
    igates = gates_in[:, :, 0, :]
    forget = jax.nn.log_sigmoid(gates_in[:, :, 1, :])
    position = jnp.arange(proposals, dtype=jnp.int32)
    within = position[None, None, :] < accepted.astype(jnp.int32)[:, None, None]
    masked = jnp.where(within, forget, 0.0)
    summed = lax.optimization_barrier(jnp.sum(masked, axis=-1))
    log_weight = jnp.where(within, summed[..., None] - jnp.cumsum(masked, axis=-1) + igates, -jnp.inf)
    carried_m = jnp.maximum(summed + state_m, lax.optimization_barrier(jnp.max(log_weight, axis=-1)))
    shrink = jnp.exp(summed + state_m - carried_m)
    weights = jnp.exp(log_weight - carried_m[..., None])
    carried_c = shrink[..., None, None] * state_c + jnp.einsum('bhs,bhsv,bhsd->bhvd', weights, values_f, scaled, precision=HIGHEST)
    carried_n = shrink[..., None] * state_n + jnp.einsum('bhs,bhsd->bhd', weights, scaled, precision=HIGHEST)
    return (carried_c, carried_n, carried_m)

def cell_block(state_c, state_n, state_m, queries, scaled, values_f, igates, forget):
    proposals = queries.shape[2]
    cumul = jnp.cumsum(forget, axis=-1)
    causal = jnp.tril(jnp.ones((proposals, proposals), dtype=bool))
    log_decay = jnp.where(causal, cumul[..., :, None] - cumul[..., None, :] + igates[..., None, :], -jnp.inf)
    carried = cumul + state_m[..., None]
    stable = jnp.maximum(carried, lax.optimization_barrier(jnp.max(log_decay, axis=-1)))
    scores = jnp.einsum('bhtd,bhsd->bhts', queries, scaled, precision=HIGHEST) * jnp.exp(log_decay - stable[..., None])
    weight_state = jnp.exp(carried - stable)
    numer = weight_state[..., None] * jnp.einsum('bhvd,bhtd->bhtv', state_c, queries, precision=HIGHEST)
    numer = numer + jnp.einsum('bhts,bhsv->bhtv', scores, values_f, precision=HIGHEST)
    denom = weight_state * jnp.einsum('bhd,bhtd->bht', state_n, queries, precision=HIGHEST) + lax.optimization_barrier(jnp.sum(scores, axis=-1))
    return numer / jnp.maximum(jnp.abs(denom), jnp.exp(-stable))[..., None]

def gate_heads(hidden, gain, outgate):
    heads_count = hidden.shape[1]
    head_size = hidden.shape[3]
    normed = hidden * lax.rsqrt(lax.optimization_barrier(jnp.mean(hidden * hidden, axis=-1, keepdims=True)) + EPSILON)
    normed = normed * gain.astype(jnp.float32).reshape(heads_count, head_size)[None, :, None, :]
    rows_out = jnp.transpose(normed, (0, 2, 1, 3)).reshape(outgate.shape)
    return (rows_out * jax.nn.sigmoid(outgate.astype(jnp.float32))).astype(jnp.bfloat16)

def reference(tokens, norm_gain, query_weight, key_weight, value_weight, outgate_weight, gate_weight, gate_bias, head_gain, out_weight, state_c, state_n, state_m, prev_keys, prev_values, prev_gates, accepted):
    batch_count = tokens.shape[0]
    tokens_f = tokens.astype(jnp.float32)
    normed = tokens_f * lax.rsqrt(lax.optimization_barrier(jnp.mean(tokens_f * tokens_f, axis=-1, keepdims=True)) + EPSILON)
    normed = (normed * norm_gain.astype(jnp.float32)).astype(jnp.bfloat16)
    rows_in = normed.reshape(batch_count * PROPS, D)

    def project(matrix):
        return jnp.dot(rows_in, matrix, preferred_element_type=jnp.float32).astype(jnp.bfloat16)

    def by_head(array):
        return array.reshape(batch_count, PROPS, HEADS, DH).transpose(0, 2, 1, 3)
    queries = project(query_weight)
    step_keys = by_head(project(key_weight))
    step_values = by_head(project(value_weight))
    outgate = project(outgate_weight)
    all_gates = jnp.dot(rows_in, gate_weight, preferred_element_type=jnp.float32) + gate_bias.reshape(-1)[None, :]
    igates = all_gates[:, :HEADS].reshape(batch_count, PROPS, HEADS).transpose(0, 2, 1)
    fgates = all_gates[:, HEADS:].reshape(batch_count, PROPS, HEADS).transpose(0, 2, 1)
    step_gates = jnp.stack([igates, fgates], axis=2)
    carried_c, carried_n, carried_m = replay(state_c, state_n, state_m, prev_keys, prev_values, prev_gates, accepted)
    hidden = cell_block(carried_c, carried_n, carried_m, by_head(queries).astype(jnp.float32), step_keys.astype(jnp.float32) * DH ** (-0.5), step_values.astype(jnp.float32), igates, jax.nn.log_sigmoid(fgates))
    gated = gate_heads(hidden, head_gain, outgate)
    mixed = jnp.dot(gated, out_weight, preferred_element_type=jnp.float32).astype(jnp.bfloat16)
    mixed = mixed.reshape(batch_count, PROPS, D)
    return (mixed, carried_c, carried_n, carried_m, step_keys, step_values, step_gates)
```

```python
import jax
import jax.numpy as jnp
from jax import lax
from jax.sharding import PartitionSpec as P

EPSILON = 1e-06
HIGHEST = lax.Precision.HIGHEST


def ring(count, step):
    return [(i, (i + step) % count) for i in range(count)]


def cores_apart(kv, tp):
    return [[(chip * 2 + core) * tp + x for chip in range(kv // 2) for x in range(tp)] for core in (0, 1)]


def gather_weight(weight):
    tp = lax.axis_size("tp")
    me = lax.axis_index("tp")
    full = jnp.zeros((tp, *weight.shape), weight.dtype)
    full = lax.dynamic_update_index_in_dim(full, weight, me, 0)
    for step in range(1, tp):
        part = lax.ppermute(weight, "tp", ring(tp, step))
        full = lax.dynamic_update_index_in_dim(full, part, lax.rem(me - step + tp, tp), 0)
    return full


def project_out(gated, weight):
    kv, tp = lax.axis_size("kv"), lax.axis_size("tp")
    chips = kv // 2
    rows = gated.shape[0] // tp
    sent = jnp.broadcast_to(gated.reshape(1, tp, rows, -1), (chips, tp, rows, gated.shape[1]))
    sent = sent.reshape(chips * tp, rows, -1)
    own = lax.all_to_all(
        sent, ("kv", "tp"), 0, 0, tiled=True, axis_index_groups=cores_apart(kv, tp)
    )
    swap = [(i, i ^ 1) for i in range(kv)]
    other = lax.ppermute(own, "kv", swap)

    def times(part):
        part = part.reshape(chips, tp, rows, -1)
        return jnp.einsum(
            "zxrk,xkn->zrn", part, weight, preferred_element_type=jnp.float32
        ).astype(jnp.bfloat16)

    first, second = times(own), times(other)
    core = lax.rem(lax.axis_index("kv"), 2)
    even = jnp.where(core == 0, first, second)
    odd = jnp.where(core == 0, second, first)
    mine = jnp.stack([even, odd], axis=1)
    everyone = lax.all_gather(mine, "tp", axis=0)
    return everyone.transpose(1, 2, 0, 3, 4).reshape(-1, weight.shape[2])


def replay(state_c, state_n, state_m, keys_in, values_in, gates_in, accepted):
    proposals = keys_in.shape[2]
    scaled = keys_in.astype(jnp.float32) * keys_in.shape[3] ** (-0.5)
    values_f = values_in.astype(jnp.float32)
    igates = gates_in[:, :, 0, :]
    forget = jax.nn.log_sigmoid(gates_in[:, :, 1, :])
    position = jnp.arange(proposals, dtype=jnp.int32)
    within = position[None, None, :] < accepted[:, None, None]
    masked = jnp.where(within, forget, 0.0)
    summed = jnp.sum(masked, axis=-1)
    log_weight = jnp.where(
        within, summed[..., None] - jnp.cumsum(masked, axis=-1) + igates, -jnp.inf
    )
    carried_m = jnp.maximum(summed + state_m, jnp.max(log_weight, axis=-1))
    shrink = jnp.exp(summed + state_m - carried_m)
    weights = jnp.exp(log_weight - carried_m[..., None])
    carried_c = shrink[..., None, None] * state_c + jnp.einsum(
        "bhs,bhsv,bhsd->bhvd", weights, values_f, scaled, precision=HIGHEST
    )
    carried_n = shrink[..., None] * state_n + jnp.einsum(
        "bhs,bhsd->bhd", weights, scaled, precision=HIGHEST
    )
    return (carried_c, carried_n, carried_m)


def cell_block(state_c, state_n, state_m, queries, scaled, values_f, igates, forget):
    proposals = queries.shape[2]
    cumul = jnp.cumsum(forget, axis=-1)
    causal = jnp.tril(jnp.ones((proposals, proposals), dtype=bool))
    log_decay = jnp.where(
        causal, cumul[..., :, None] - cumul[..., None, :] + igates[..., None, :], -jnp.inf
    )
    carried = cumul + state_m[..., None]
    stable = jnp.maximum(carried, jnp.max(log_decay, axis=-1))
    scores = jnp.einsum("bhtd,bhsd->bhts", queries, scaled, precision=HIGHEST) * jnp.exp(
        log_decay - stable[..., None]
    )
    weight_state = jnp.exp(carried - stable)
    numer = weight_state[..., None] * jnp.einsum(
        "bhvd,bhtd->bhtv", state_c, queries, precision=HIGHEST
    )
    numer = numer + jnp.einsum("bhts,bhsv->bhtv", scores, values_f, precision=HIGHEST)
    denom = weight_state * jnp.einsum(
        "bhd,bhtd->bht", state_n, queries, precision=HIGHEST
    ) + jnp.sum(scores, axis=-1)
    return numer / jnp.maximum(jnp.abs(denom), jnp.exp(-stable))[..., None]


def gate_heads(hidden, gain, outgate):
    heads_count = hidden.shape[1]
    head_size = hidden.shape[3]
    normed = hidden * lax.rsqrt(jnp.mean(hidden * hidden, axis=-1, keepdims=True) + EPSILON)
    normed = normed * gain.astype(jnp.float32).reshape(heads_count, head_size)[None, :, None, :]
    rows_out = jnp.transpose(normed, (0, 2, 1, 3)).reshape(outgate.shape)
    return (rows_out * jax.nn.sigmoid(outgate.astype(jnp.float32))).astype(jnp.bfloat16)


def per_device(
    tokens,
    norm_gain,
    query_weight,
    key_weight,
    value_weight,
    outgate_weight,
    gate_weight,
    gate_bias,
    head_gain,
    out_weight,
    state_c,
    state_n,
    state_m,
    prev_keys,
    prev_values,
    prev_gates,
    accepted,
):
    seqs_local, proposals, features = tokens.shape
    heads_local = state_m.shape[1]
    head_size = state_n.shape[2]
    tokens_f = tokens.astype(jnp.float32)
    normed = tokens_f * lax.rsqrt(jnp.mean(tokens_f * tokens_f, axis=-1, keepdims=True) + EPSILON)
    normed = (normed * norm_gain.astype(jnp.float32)).astype(jnp.bfloat16)
    rows_in = normed.reshape(seqs_local * proposals, features)

    def project(matrix):
        return jnp.dot(rows_in, matrix, preferred_element_type=jnp.float32).astype(jnp.bfloat16)

    def by_head(array):
        return array.reshape(seqs_local, proposals, heads_local, head_size).transpose(0, 2, 1, 3)

    queries = project(query_weight)
    keys_new = project(key_weight)
    values_new = project(value_weight)
    outgate = project(outgate_weight)
    all_gates = (
        jnp.dot(rows_in, gate_weight, preferred_element_type=jnp.float32)
        + gate_bias.reshape(-1)[None, :]
    )
    heads_total = gate_weight.shape[1] // 2
    head_offset = lax.axis_index("tp") * heads_local
    igates = lax.dynamic_slice_in_dim(all_gates, head_offset, heads_local, 1)
    fgates = lax.dynamic_slice_in_dim(all_gates, heads_total + head_offset, heads_local, 1)
    igates = igates.reshape(seqs_local, proposals, heads_local).transpose(0, 2, 1)
    fgates = fgates.reshape(seqs_local, proposals, heads_local).transpose(0, 2, 1)
    step_gates = jnp.stack([igates, fgates], axis=2)
    carried_c, carried_n, carried_m = replay(
        state_c, state_n, state_m, prev_keys, prev_values, prev_gates, accepted
    )
    step_keys = by_head(keys_new)
    step_values = by_head(values_new)
    hidden = cell_block(
        carried_c,
        carried_n,
        carried_m,
        by_head(queries).astype(jnp.float32),
        step_keys.astype(jnp.float32) * head_size ** (-0.5),
        step_values.astype(jnp.float32),
        igates,
        jax.nn.log_sigmoid(fgates),
    )
    gated = gate_heads(hidden, head_gain, outgate)
    mixed = project_out(gated, gather_weight(out_weight))
    mixed = mixed.reshape(-1, proposals, mixed.shape[1])
    return (mixed, carried_c, carried_n, carried_m, step_keys, step_values, step_gates)


def solution(mesh):
    in_specs = (
        P("kv", None, None),
        P(),
        P(None, "tp"),
        P(None, "tp"),
        P(None, "tp"),
        P(None, "tp"),
        P(),
        P(),
        P("tp"),
        P("tp", "kv"),
        P("kv", "tp", None, None),
        P("kv", "tp", None),
        P("kv", "tp"),
        P("kv", "tp", None, None),
        P("kv", "tp", None, None),
        P("kv", "tp", None, None),
        P("kv"),
    )
    out_specs = (
        P(None, None, "kv"),
        P("kv", "tp", None, None),
        P("kv", "tp", None),
        P("kv", "tp"),
        P("kv", "tp", None, None),
        P("kv", "tp", None, None),
        P("kv", "tp", None, None),
    )
    return jax.shard_map(
        per_device, mesh=mesh, in_specs=in_specs, out_specs=out_specs, check_vma=False
    )
```

```python
import jax
import jax.numpy as jnp
from jax import lax
from jax.experimental import pallas as pl
from jax.experimental.pallas import tpu as pltpu
from jax.sharding import PartitionSpec as P


EPSILON = 1e-06
HIGHEST = lax.Precision.HIGHEST


def ring(count, step):
    return [(i, (i + step) % count) for i in range(count)]


def swap_cores(x):
    return lax.ppermute(x, "kv", [(i, i ^ 1) for i in range(lax.axis_size("kv"))])


def passed_on(weight):
    tp = lax.axis_size("tp")
    return [weight] + [lax.ppermute(weight, "tp", ring(tp, step)) for step in range(1, tp)]


def mix_kernel(received, *refs):
    weights, out = refs[:-1], refs[-1]
    chips, tp, rows, depth = received.shape
    me = lax.axis_index("tp")
    core = lax.rem(lax.axis_index("kv"), 2)
    total = None
    for step in range(tp):
        source = lax.rem(me - step + tp, tp)
        part = received[:, pl.ds(source, 1)].reshape(chips * rows, depth)
        both = jnp.concatenate([weights[step][...], weights[tp + step][...]], axis=1)
        dot = jnp.dot(part, both, preferred_element_type=jnp.float32)
        total = dot if total is None else total + dot
    mixed = total.astype(jnp.bfloat16)
    columns = mixed.shape[1] // 2
    for x in range(tp):
        out[core, x] = mixed[:, :columns]
        out[1 - core, x] = mixed[:, columns:]


def same_core(kv, tp):
    return [
        [(chip * 2 + core) * tp + x for chip in range(kv // 2) for x in range(tp)]
        for core in (0, 1)
    ]


def same_line(kv, tp):
    return [
        [(chip * 2 + core) * tp + x for core in (0, 1) for x in range(tp)]
        for chip in range(kv // 2)
    ]


def project_out(sent, own_parts):
    kv, tp = lax.axis_size("kv"), lax.axis_size("tp")
    chips = kv // 2
    rows, depth = sent.shape[1] // tp, sent.shape[2]
    other_parts = [swap_cores(part) for part in own_parts]
    received = lax.all_to_all(
        sent.reshape(chips * tp, rows, depth), ("kv", "tp"), 0, 0,
        tiled=True, axis_index_groups=same_core(kv, tp),
    ).reshape(chips, tp, rows, depth)
    columns = own_parts[0].shape[1]
    mixed = pl.pallas_call(
        mix_kernel,
        out_shape=jax.ShapeDtypeStruct((2, tp, chips * rows, columns), jnp.bfloat16),
        compiler_params=pltpu.CompilerParams(vmem_limit_bytes=12 * 1024 * 1024),
        cost_estimate=pl.CostEstimate(
            flops=4 * chips * rows * tp * depth * columns,
            bytes_accessed=3 << 20,
            transcendentals=0,
        ),
    )(received, *own_parts, *other_parts)
    everyone = lax.all_to_all(
        mixed.reshape(2 * tp, chips * rows, columns), ("kv", "tp"), 0, 0,
        tiled=True, axis_index_groups=same_line(kv, tp),
    ).reshape(2, tp, chips, rows, columns)
    return everyone.transpose(2, 0, 1, 3, 4).reshape(-1, columns)


def split(x):
    high = x.astype(jnp.bfloat16)
    return high, (x - high.astype(jnp.float32)).astype(jnp.bfloat16)


def exact_dot(a, b, contract):
    return lax.dot_general(
        a, b, ((contract[:1], contract[1:]), ((), ())),
        precision=HIGHEST, preferred_element_type=jnp.float32,
    )


def dot_nt(a, b):
    return lax.dot_general(
        a, b, (((1,), (1,)), ((), ())), preferred_element_type=jnp.float32
    )


def log_sigmoid(x):
    return jnp.minimum(x, 0.0) - jnp.log1p(jnp.exp(-jnp.abs(x)))


def iota(shape, dim):
    return lax.broadcasted_iota(jnp.int32, shape, dim)


def cell_kernel(
    accepted,
    tokens,
    norm_gain,
    query_weight,
    key_weight,
    value_weight,
    outgate_weight,
    gate_weight,
    gate_bias,
    head_gain,
    state_c,
    state_n,
    state_m,
    prev_keys,
    prev_values,
    prev_gates,
    gated_out,
    carried_c,
    carried_n,
    carried_m,
    step_keys,
    step_values,
    step_gates,
    tokens_v,
    gain_v,
    weights_v,
    gate_weight_v,
    gate_bias_v,
    head_gain_v,
    state_c_v,
    state_n_v,
    state_m_v,
    prev_keys_v,
    prev_values_v,
    prev_gates_v,
    normed_f,
    normed_v,
    recall_v,
    gated_v,
    sems,
    out_sems,
):
    f32, bf16 = jnp.float32, jnp.bfloat16
    seqs, props, width = tokens_v.shape
    heads, _, size, _ = state_c_v.shape
    rows = seqs * props
    heads_total = gate_weight_v.shape[0] // 2
    scale = size ** (-0.5)
    pieces = 4
    depth = width // pieces

    copies = []

    def bring(src, dst):
        copy = pltpu.make_async_copy(src, dst, sems.at[len(copies)])
        copies.append(copy)
        copy.start()
        return copy

    def bring_weight(which, src):
        return [
            bring(src.at[pl.ds(p * depth, depth)], weights_v.at[which, pl.ds(p * depth, depth)])
            for p in range(pieces)
        ]

    early = [bring(tokens, tokens_v), bring(norm_gain, gain_v)]
    gates_in = [bring(gate_weight, gate_weight_v), bring(gate_bias, gate_bias_v)]
    replay_in = [
        bring(state_m, state_m_v),
        bring(prev_gates, prev_gates_v),
        bring(state_n, state_n_v),
        bring(prev_keys, prev_keys_v),
        bring(prev_values, prev_values_v),
        bring(head_gain, head_gain_v),
    ]
    weights_in = [bring_weight(0, query_weight)]
    states_in = [bring(state_c.at[:, h], state_c_v.at[h]) for h in range(heads)]
    weights_in += [
        bring_weight(1, key_weight),
        bring_weight(2, value_weight),
        bring_weight(3, outgate_weight),
    ]

    def arrive(some):
        for copy in some:
            copy.wait()

    row_lane = iota((1, rows), 1)
    prop_lane = row_lane & (props - 1)
    spread = jnp.where(iota((seqs, rows), 0) == (iota((seqs, rows), 1) >> 2), 1.0, 0.0)
    spread_t = jnp.where((iota((rows, seqs), 0) >> 2) == iota((rows, seqs), 1), 1.0, 0.0)
    square = (rows, rows)
    same = (iota(square, 0) >> 2) == (iota(square, 1) >> 2)
    causal = same & (iota(square, 0) >= iota(square, 1))

    arrive(early)
    gain = gain_v[...].astype(f32)
    for b in range(seqs):
        x = tokens_v[b].astype(f32)
        mean = jnp.mean(x * x, axis=-1, keepdims=True)
        normed_f[b * props : (b + 1) * props, :] = x * lax.rsqrt(mean + EPSILON) * gain
    normed_v[...] = normed_f[...].astype(bf16)

    arrive(gates_in)
    bias = jnp.concatenate([gate_bias_v[0:1, :], gate_bias_v[1:2, :]], axis=1)
    gates = dot_nt(normed_v[...], gate_weight_v[...]) + bias
    gates = jnp.concatenate([gates, jnp.zeros((rows, 128 - 2 * heads_total), f32)], axis=1)
    first_head = lax.axis_index("tp") * heads
    gates = pltpu.roll(gates, 128 - first_head, 1)
    forget = log_sigmoid(gates)
    cumul = exact_dot(jnp.where(causal, 1.0, 0.0), forget, (1, 0))
    gates_t = gates.T
    cumul_t = cumul.T
    for t in range(props):
        pick = jnp.where(iota((rows, seqs), 0) == iota((rows, seqs), 1) * props + t, 1.0, 0.0)
        picked = exact_dot(gates_t[: 2 * heads_total], pick, (1, 0))
        for h in range(heads):
            step_gates[h, 0, t : t + 1, :] = picked[h : h + 1, :]
            step_gates[h, 1, t : t + 1, :] = picked[heads_total + h : heads_total + h + 1, :]

    arrive(replay_in)
    seq_lane = iota((1, seqs), 1)
    counts = jnp.zeros((1, seqs), jnp.int32)
    for b in range(seqs):
        counts = jnp.where(seq_lane == b, accepted[b], counts)
    total = jnp.zeros((heads, seqs), f32)
    sums, inputs = [], []
    for s in range(props):
        both = [
            jnp.concatenate([prev_gates_v[h, g, s : s + 1, :] for h in range(heads)], axis=0)
            for g in (0, 1)
        ]
        total = total + jnp.where(counts > s, log_sigmoid(both[1]), 0.0)
        sums.append(total)
        inputs.append(both[0])
    logs = [
        jnp.where(counts > s, total - sums[s] + inputs[s], -jnp.inf) for s in range(props)
    ]
    decayed = total + state_m_v[...]
    stable = decayed
    for s in range(props):
        stable = jnp.maximum(stable, logs[s])
    carried_m[...] = stable
    shrink = jnp.exp(decayed - stable)
    weights = jnp.zeros((heads, rows), f32)
    for s in range(props):
        spaced = exact_dot(jnp.exp(logs[s] - stable), spread, (1, 0))
        weights = weights + jnp.where(prop_lane == s, spaced, 0.0)
    weights = weights * scale
    stable_col = exact_dot(spread_t, stable, (1, 1))
    diagonal = jnp.where(iota((seqs, seqs), 0) == iota((seqs, seqs), 1), 1.0, 0.0)
    shrink_col = exact_dot(diagonal, shrink, (1, 1))

    def project(which):
        acc = None
        for p in range(pieces):
            weights_in[which][p].wait()
            part = jnp.dot(
                normed_v[:, p * depth : (p + 1) * depth],
                weights_v[which, p * depth : (p + 1) * depth, :],
                preferred_element_type=f32,
            )
            acc = part if acc is None else acc + part
        return acc.astype(bf16)

    queries = project(0)
    out_copies = []
    seq_of_lane = (iota((1, 2 * rows), 1) & (rows - 1)) >> 2
    upper = iota((2 * props, size), 0) < props
    recall_norm = []
    for h in range(heads):
        cols = slice(h * size, (h + 1) * size)
        query = queries[:, cols]
        query_f = query.astype(f32)
        keys = prev_keys_v[:, h].astype(f32).reshape(rows, size)
        values = prev_values_v[:, h].astype(f32).reshape(rows, size)
        weight = weights[h : h + 1, :]
        norm = shrink_col[:, h : h + 1] * state_n_v[:, h, :] + exact_dot(
            spread * weight, keys, (1, 0)
        )
        carried_n[:, h, :] = norm
        along = exact_dot(query_f, norm, (1, 1))
        recall_norm.append(jnp.sum(along * spread_t, axis=1, keepdims=True))
        weighted = jnp.concatenate(split(values.T * weight), axis=1)
        key_pair = jnp.concatenate([keys, keys], axis=0).astype(bf16)
        states_in[h].wait()
        for p in range(seqs // 2):
            stacked = []
            for b in (2 * p, 2 * p + 1):
                mask = jnp.where(seq_of_lane == b, 1.0, 0.0).astype(bf16)
                update = jnp.dot(weighted * mask, key_pair, preferred_element_type=f32)
                state = shrink[h : h + 1, b : b + 1] * state_c_v[h, b] + update
                state_c_v[h, b] = state
                stacked.append(jnp.concatenate(split(state), axis=1))
            pair = slice(2 * p * props, 2 * (p + 1) * props)
            asked = query_f[pair].astype(bf16)
            found = dot_nt(
                jnp.concatenate([asked, asked], axis=1), jnp.concatenate(stacked, axis=0)
            )
            recall_v[pair, cols] = jnp.where(upper, found[:, :size], found[:, size:])
        copy = pltpu.make_async_copy(state_c_v.at[h], carried_c.at[:, h], out_sems.at[h])
        copy.start()
        out_copies.append(copy)

    new_keys = project(1)
    new_values = project(2)
    outgate = project(3)
    for h in range(heads):
        cols = slice(h * size, (h + 1) * size)
        query, key, value = queries[:, cols], new_keys[:, cols], new_values[:, cols]
        step_keys[:, h] = key.astype(f32).reshape(seqs, props, size).astype(bf16)
        step_values[:, h] = value.astype(f32).reshape(seqs, props, size).astype(bf16)
        c_col = cumul[:, heads_total + h : heads_total + h + 1]
        c_row = cumul_t[heads_total + h : heads_total + h + 1, :]
        i_row = gates_t[h : h + 1, :]
        logs_ts = jnp.where(causal, c_col - c_row + i_row, -jnp.inf)
        carried = c_col + stable_col[:, h : h + 1]
        steady = jnp.maximum(carried, jnp.max(logs_ts, axis=1, keepdims=True))
        scores = dot_nt(query, key) * scale * jnp.exp(logs_ts - steady)
        weight_state = jnp.exp(carried - steady)
        numer = weight_state * recall_v[:, cols] + jnp.dot(
            jnp.concatenate(split(scores), axis=1),
            jnp.concatenate([value, value], axis=0),
            preferred_element_type=f32,
        )
        denom = weight_state * recall_norm[h] + jnp.sum(scores, axis=1, keepdims=True)
        hidden = numer / jnp.maximum(jnp.abs(denom), jnp.exp(-steady))
        hidden = hidden * lax.rsqrt(jnp.mean(hidden * hidden, axis=1, keepdims=True) + EPSILON)
        hidden = hidden * head_gain_v[:, cols].astype(f32)
        gated_v[:, cols] = (hidden * jax.nn.sigmoid(outgate[:, cols].astype(f32))).astype(bf16)
    for chip in range(gated_out.shape[0]):
        copy = pltpu.make_async_copy(gated_v, gated_out.at[chip], out_sems.at[len(out_copies)])
        copy.start()
        out_copies.append(copy)
    arrive(out_copies)


def cell(
    tokens, norm_gain, query_weight, key_weight, value_weight, outgate_weight, gate_weight,
    gate_bias, head_gain, state_c, state_n, state_m, prev_keys, prev_values, prev_gates, accepted,
):
    f32, bf16 = jnp.float32, jnp.bfloat16
    seqs, props, width = tokens.shape
    heads, size = state_n.shape[1:]
    rows, columns = seqs * props, heads * size
    chips = lax.axis_size("kv") // 2
    inputs = (
        accepted,
        tokens,
        norm_gain.reshape(1, width),
        query_weight,
        key_weight,
        value_weight,
        outgate_weight,
        gate_weight.T,
        gate_bias,
        head_gain.reshape(1, columns),
        state_c,
        state_n,
        state_m.T,
        prev_keys,
        prev_values,
        prev_gates.transpose(1, 2, 3, 0),
    )
    outs = (
        jax.ShapeDtypeStruct((chips, rows, columns), bf16),
        jax.ShapeDtypeStruct(state_c.shape, f32),
        jax.ShapeDtypeStruct(state_n.shape, f32),
        jax.ShapeDtypeStruct((heads, seqs), f32),
        jax.ShapeDtypeStruct(prev_keys.shape, bf16),
        jax.ShapeDtypeStruct(prev_values.shape, bf16),
        jax.ShapeDtypeStruct((heads, 2, props, seqs), f32),
    )
    here = pl.BlockSpec(memory_space=pltpu.VMEM)
    anywhere = pl.BlockSpec(memory_space=pltpu.HBM)
    outputs = pl.pallas_call(
        cell_kernel,
        out_shape=outs,
        in_specs=[pl.BlockSpec(memory_space=pltpu.SMEM)] + [anywhere] * 15,
        out_specs=[anywhere, anywhere] + [here] * 5,
        scratch_shapes=[
            pltpu.VMEM(tokens.shape, bf16),
            pltpu.VMEM((1, width), bf16),
            pltpu.VMEM((4, width, columns), bf16),
            pltpu.VMEM(gate_weight.shape[::-1], bf16),
            pltpu.VMEM(gate_bias.shape, f32),
            pltpu.VMEM((1, columns), bf16),
            pltpu.VMEM((heads, seqs, size, size), f32),
            pltpu.VMEM(state_n.shape, f32),
            pltpu.VMEM((heads, seqs), f32),
            pltpu.VMEM(prev_keys.shape, bf16),
            pltpu.VMEM(prev_values.shape, bf16),
            pltpu.VMEM((heads, 2, props, seqs), f32),
            pltpu.VMEM((rows, width), f32),
            pltpu.VMEM((rows, width), bf16),
            pltpu.VMEM((rows, columns), f32),
            pltpu.VMEM((rows, columns), bf16),
            pltpu.SemaphoreType.DMA((10 + 16 + heads,)),
            pltpu.SemaphoreType.DMA((heads + chips,)),
        ],
        compiler_params=pltpu.CompilerParams(vmem_limit_bytes=62 * 1024 * 1024),
        cost_estimate=pl.CostEstimate(
            flops=2 * rows * width * 4 * columns, bytes_accessed=27 << 20, transcendentals=0
        ),
    )(*inputs)
    gated, new_c, new_n, new_m, keys, values, gates = outputs
    return gated, new_c, new_n, new_m.T, keys, values, gates.transpose(3, 0, 1, 2)


def per_device(*arrays):
    inputs, out_weight = arrays[:9] + arrays[10:], arrays[9]
    parts = passed_on(out_weight)
    sent, *rest = cell(*inputs)
    mixed = project_out(sent, parts)
    return (mixed.reshape(-1, inputs[0].shape[1], mixed.shape[1]), *rest)


def solution(mesh):
    in_specs = (
        P("kv", None, None),
        P(),
        P(None, "tp"),
        P(None, "tp"),
        P(None, "tp"),
        P(None, "tp"),
        P(),
        P(),
        P("tp"),
        P("tp", "kv"),
        P("kv", "tp", None, None),
        P("kv", "tp", None),
        P("kv", "tp"),
        P("kv", "tp", None, None),
        P("kv", "tp", None, None),
        P("kv", "tp", None, None),
        P("kv"),
    )
    out_specs = (
        P(None, None, "kv"),
        P("kv", "tp", None, None),
        P("kv", "tp", None),
        P("kv", "tp"),
        P("kv", "tp", None, None),
        P("kv", "tp", None, None),
        P("kv", "tp", None, None),
    )
    return jax.shard_map(
        per_device, mesh=mesh, in_specs=in_specs, out_specs=out_specs, check_vma=False
    )
```

```python
import jax
import jax.numpy as jnp
from jax import lax
from jax.experimental import pallas as pl
from jax.experimental.pallas import tpu as pltpu
from jax.sharding import PartitionSpec as P


EPSILON = 1e-06
HIGHEST = lax.Precision.HIGHEST


def ring(count, step):
    return [(i, (i + step) % count) for i in range(count)]


def swap_cores(x):
    return lax.ppermute(x, "kv", [(i, i ^ 1) for i in range(lax.axis_size("kv"))])


def passed_on(weight):
    tp = lax.axis_size("tp")
    return [weight] + [lax.ppermute(weight, "tp", ring(tp, step)) for step in range(1, tp)]


def mix_kernel(received, *refs):
    weights, out = refs[:-1], refs[-1]
    chips, tp, rows, depth = received.shape
    me = lax.axis_index("tp")
    core = lax.rem(lax.axis_index("kv"), 2)
    total = None
    for step in range(tp):
        source = lax.rem(me - step + tp, tp)
        part = received[:, pl.ds(source, 1)].reshape(chips * rows, depth)
        both = jnp.concatenate([weights[step][...], weights[tp + step][...]], axis=1)
        dot = jnp.dot(part, both, preferred_element_type=jnp.float32)
        total = dot if total is None else total + dot
    mixed = total.astype(jnp.bfloat16)
    columns = mixed.shape[1] // 2
    for x in range(tp):
        out[core, x] = mixed[:, :columns]
        out[1 - core, x] = mixed[:, columns:]


def same_core(kv, tp):
    return [
        [(chip * 2 + core) * tp + x for chip in range(kv // 2) for x in range(tp)]
        for core in (0, 1)
    ]


def same_line(kv, tp):
    return [
        [(chip * 2 + core) * tp + x for core in (0, 1) for x in range(tp)]
        for chip in range(kv // 2)
    ]


def project_out(sent, own_parts):
    kv, tp = lax.axis_size("kv"), lax.axis_size("tp")
    chips = kv // 2
    rows, depth = sent.shape[1] // tp, sent.shape[2]
    other_parts = [swap_cores(part) for part in own_parts]
    received = lax.all_to_all(
        sent.reshape(chips * tp, rows, depth), ("kv", "tp"), 0, 0,
        tiled=True, axis_index_groups=same_core(kv, tp),
    ).reshape(chips, tp, rows, depth)
    columns = own_parts[0].shape[1]
    mixed = pl.pallas_call(
        mix_kernel,
        out_shape=jax.ShapeDtypeStruct((2, tp, chips * rows, columns), jnp.bfloat16),
        compiler_params=pltpu.CompilerParams(vmem_limit_bytes=12 * 1024 * 1024),
        cost_estimate=pl.CostEstimate(
            flops=4 * chips * rows * tp * depth * columns,
            bytes_accessed=3 << 20,
            transcendentals=0,
        ),
    )(received, *own_parts, *other_parts)
    everyone = lax.all_to_all(
        mixed.reshape(2 * tp, chips * rows, columns), ("kv", "tp"), 0, 0,
        tiled=True, axis_index_groups=same_line(kv, tp),
    ).reshape(2, tp, chips, rows, columns)
    return everyone.transpose(2, 0, 1, 3, 4).reshape(-1, columns)


def split(x):
    high = x.astype(jnp.bfloat16)
    return high, (x - high.astype(jnp.float32)).astype(jnp.bfloat16)


def exact_dot(a, b, contract):
    return lax.dot_general(
        a, b, ((contract[:1], contract[1:]), ((), ())),
        precision=HIGHEST, preferred_element_type=jnp.float32,
    )


def dot_nt(a, b):
    return lax.dot_general(
        a, b, (((1,), (1,)), ((), ())), preferred_element_type=jnp.float32
    )


def log_sigmoid(x):
    return jnp.minimum(x, 0.0) - jnp.log1p(jnp.exp(-jnp.abs(x)))


def iota(shape, dim):
    return lax.broadcasted_iota(jnp.int32, shape, dim)


def bringer(sems):
    copies = []

    def bring(src, dst):
        copy = pltpu.make_async_copy(src, dst, sems.at[len(copies)])
        copies.append(copy)
        copy.start()
        return copy

    return bring


def arrive(some):
    for copy in some:
        copy.wait()


def spreads(seqs, rows):
    across = jnp.where(iota((seqs, rows), 0) == (iota((seqs, rows), 1) >> 2), 1.0, 0.0)
    down = jnp.where((iota((rows, seqs), 0) >> 2) == iota((rows, seqs), 1), 1.0, 0.0)
    return across, down


def replay(accepted, state_m, prev_gates, across):
    heads, _, props, seqs = prev_gates.shape
    seq_lane = iota((1, seqs), 1)
    counts = jnp.zeros((1, seqs), jnp.int32)
    for b in range(seqs):
        counts = jnp.where(seq_lane == b, accepted[b], counts)
    total = jnp.zeros((heads, seqs), jnp.float32)
    sums, inputs = [], []
    for s in range(props):
        both = [
            jnp.concatenate([prev_gates[h, g, s : s + 1, :] for h in range(heads)], axis=0)
            for g in (0, 1)
        ]
        total = total + jnp.where(counts > s, log_sigmoid(both[1]), 0.0)
        sums.append(total)
        inputs.append(both[0])
    logs = [
        jnp.where(counts > s, total - sums[s] + inputs[s], -jnp.inf) for s in range(props)
    ]
    decayed = total + state_m[...]
    stable = decayed
    for s in range(props):
        stable = jnp.maximum(stable, logs[s])
    shrink = jnp.exp(decayed - stable)
    prop_lane = iota((1, across.shape[1]), 1) & (props - 1)
    weights = jnp.zeros((heads, across.shape[1]), jnp.float32)
    for s in range(props):
        spaced = exact_dot(jnp.exp(logs[s] - stable), across, (1, 0))
        weights = weights + jnp.where(prop_lane == s, spaced, 0.0)
    return stable, shrink, weights


def cell_kernel(
    accepted,
    tokens,
    norm_gain,
    query_weight,
    key_weight,
    value_weight,
    outgate_weight,
    gate_weight,
    gate_bias,
    head_gain,
    state_c,
    state_n,
    state_m,
    prev_keys,
    prev_values,
    prev_gates,
    gated_out,
    keys_out,
    values_out,
    gates_out,
    accepted_s,
    tokens_v,
    gain_v,
    weights_v,
    gate_weight_v,
    gate_bias_v,
    head_gain_v,
    state_c_v,
    state_n_v,
    state_m_v,
    prev_keys_v,
    prev_values_v,
    prev_gates_v,
    normed_f,
    normed_v,
    recall_v,
    hidden_v,
    gated_v,
    sems,
    out_sems,
):
    f32, bf16 = jnp.float32, jnp.bfloat16
    seqs, props, width = tokens_v.shape
    heads, _, size, _ = state_c_v.shape
    rows = seqs * props
    heads_total = gate_weight_v.shape[0] // 2
    scale = size ** (-0.5)
    pieces = 4
    depth = width // pieces
    bring = bringer(sems)

    def bring_weight(which, src):
        return [
            bring(src.at[pl.ds(p * depth, depth)], weights_v.at[which, pl.ds(p * depth, depth)])
            for p in range(pieces)
        ]

    early = [bring(tokens, tokens_v), bring(norm_gain, gain_v)]
    gates_in = [bring(gate_weight, gate_weight_v), bring(gate_bias, gate_bias_v)]
    replay_in = [
        bring(accepted, accepted_s),
        bring(state_m, state_m_v),
        bring(prev_gates, prev_gates_v),
        bring(state_n, state_n_v),
        bring(prev_keys, prev_keys_v),
        bring(prev_values, prev_values_v),
        bring(head_gain, head_gain_v),
    ]
    weights_in = [bring_weight(0, query_weight)]
    states_in = [bring(state_c.at[:, h], state_c_v.at[h]) for h in range(heads)]
    weights_in += [
        bring_weight(1, key_weight),
        bring_weight(2, value_weight),
        bring_weight(3, outgate_weight),
    ]

    across, down = spreads(seqs, rows)
    square = (rows, rows)
    same = (iota(square, 0) >> 2) == (iota(square, 1) >> 2)
    causal = same & (iota(square, 0) >= iota(square, 1))

    arrive(early)
    gain = gain_v[...].astype(f32).reshape(1, width)
    for b in range(seqs):
        x = tokens_v[b].astype(f32)
        mean = jnp.mean(x * x, axis=-1, keepdims=True)
        normed_f[b * props : (b + 1) * props, :] = x * lax.rsqrt(mean + EPSILON) * gain
    normed_v[...] = normed_f[...].astype(bf16)

    arrive(gates_in)
    bias = jnp.concatenate([gate_bias_v[0:1, :], gate_bias_v[1:2, :]], axis=1)
    gates = dot_nt(normed_v[...], gate_weight_v[...]) + bias
    gates = jnp.concatenate([gates, jnp.zeros((rows, 128 - 2 * heads_total), f32)], axis=1)
    first_head = lax.axis_index("tp") * heads
    gates = pltpu.roll(gates, 128 - first_head, 1)
    cumul = exact_dot(jnp.where(causal, 1.0, 0.0), log_sigmoid(gates), (1, 0))
    gates_t = gates.T
    cumul_t = cumul.T
    gates_out[...] = gates_t[: 2 * heads_total]

    arrive(replay_in)
    stable, shrink, weights = replay(accepted_s, state_m_v, prev_gates_v, across)
    weights = weights * scale
    stable_col = exact_dot(down, stable, (1, 1))
    shrink_col = exact_dot(down, shrink, (1, 1))

    def project(which):
        acc = None
        for p in range(pieces):
            weights_in[which][p].wait()
            part = jnp.dot(
                normed_v[:, p * depth : (p + 1) * depth],
                weights_v[which, p * depth : (p + 1) * depth, :],
                preferred_element_type=f32,
            )
            acc = part if acc is None else acc + part
        return acc.astype(bf16)

    queries = project(0)
    upper = iota((2 * props, size), 0) < props
    for h in range(heads):
        cols = slice(h * size, (h + 1) * size)
        query_f = queries[:, cols].astype(f32)
        states_in[h].wait()
        for p in range(seqs // 2):
            stacked = [
                jnp.concatenate(split(state_c_v[h, b]), axis=1) for b in (2 * p, 2 * p + 1)
            ]
            pair = slice(2 * p * props, 2 * (p + 1) * props)
            asked = query_f[pair].astype(bf16)
            found = dot_nt(
                jnp.concatenate([asked, asked], axis=1), jnp.concatenate(stacked, axis=0)
            )
            recall_v[pair, cols] = jnp.where(upper, found[:, :size], found[:, size:])

    new_keys = project(1)
    keys_out[...] = new_keys
    new_values = project(2)
    values_out[...] = new_values
    for h in range(heads):
        cols = slice(h * size, (h + 1) * size)
        query, key, value = queries[:, cols], new_keys[:, cols], new_values[:, cols]
        old_key = prev_keys_v[:, h].astype(f32).reshape(rows, size).astype(bf16)
        old_value = prev_values_v[:, h].astype(f32).reshape(rows, size).astype(bf16)
        c_col = cumul[:, heads_total + h : heads_total + h + 1]
        c_row = cumul_t[heads_total + h : heads_total + h + 1, :]
        i_row = gates_t[h : h + 1, :]
        logs_ts = jnp.where(causal, c_col - c_row + i_row, -jnp.inf)
        carried = c_col + stable_col[:, h : h + 1]
        steady = jnp.maximum(carried, jnp.max(logs_ts, axis=1, keepdims=True))
        weight_state = jnp.exp(carried - steady)
        scores = dot_nt(query, key) * scale * jnp.exp(logs_ts - steady)
        replayed = jnp.where(same, dot_nt(query, old_key) * weights[h : h + 1, :], 0.0)
        both = jnp.concatenate([weight_state * replayed, scores], axis=1)
        kept = weight_state * shrink_col[:, h : h + 1]
        numer = kept * recall_v[:, cols] + jnp.dot(
            jnp.concatenate(split(both), axis=1),
            jnp.concatenate([old_value, value] * 2, axis=0),
            preferred_element_type=f32,
        )
        along = exact_dot(query.astype(f32), state_n_v[:, h, :], (1, 1))
        recall_norm = jnp.sum(along * down, axis=1, keepdims=True)
        denom = kept * recall_norm + jnp.sum(both, axis=1, keepdims=True)
        hidden = numer / jnp.maximum(jnp.abs(denom), jnp.exp(-steady))
        hidden_v[:, cols] = hidden * lax.rsqrt(
            jnp.mean(hidden * hidden, axis=1, keepdims=True) + EPSILON
        )

    outgate = project(3)
    head_scale = head_gain_v[...].astype(f32).reshape(1, heads * size)
    gated_v[...] = (
        hidden_v[...] * head_scale * jax.nn.sigmoid(outgate.astype(f32))
    ).astype(bf16)
    sends = [
        pltpu.make_async_copy(gated_v, gated_out.at[chip], out_sems.at[chip])
        for chip in range(gated_out.shape[0])
    ]
    for copy in sends:
        copy.start()
    arrive(sends)


def keep_kernel(
    accepted,
    state_c,
    state_n,
    state_m,
    prev_keys,
    prev_values,
    prev_gates,
    new_keys,
    new_values,
    gates_t,
    carried_c,
    carried_n,
    carried_m,
    step_keys,
    step_values,
    step_gates,
    state_c_v,
    sems,
    out_sems,
):
    f32, bf16 = jnp.float32, jnp.bfloat16
    heads, seqs, size, _ = state_c_v.shape
    props = prev_gates.shape[2]
    rows = seqs * props
    scale = size ** (-0.5)
    bring = bringer(sems)
    states_in = [bring(state_c.at[:, h], state_c_v.at[h]) for h in range(heads)]
    across, _ = spreads(seqs, rows)
    for t in range(props):
        pick = jnp.where(iota((rows, seqs), 0) == iota((rows, seqs), 1) * props + t, 1.0, 0.0)
        picked = exact_dot(gates_t[...], pick, (1, 0))
        total = picked.shape[0] // 2
        for h in range(heads):
            step_gates[h, 0, t : t + 1, :] = picked[h : h + 1, :]
            step_gates[h, 1, t : t + 1, :] = picked[total + h : total + h + 1, :]
    stable, shrink, weights = replay(accepted, state_m, prev_gates, across)
    weights = weights * scale
    carried_m[...] = stable
    diagonal = jnp.where(iota((seqs, seqs), 0) == iota((seqs, seqs), 1), 1.0, 0.0)
    shrink_col = exact_dot(diagonal, shrink, (1, 1))
    seq_of_lane = (iota((1, 2 * rows), 1) & (rows - 1)) >> 2
    outs = []
    for h in range(heads):
        cols = slice(h * size, (h + 1) * size)
        step_keys[:, h] = new_keys[:, cols].astype(f32).reshape(seqs, props, size).astype(bf16)
        step_values[:, h] = new_values[:, cols].astype(f32).reshape(seqs, props, size).astype(bf16)
        keys = prev_keys[:, h].astype(f32).reshape(rows, size)
        values = prev_values[:, h].astype(f32).reshape(rows, size)
        weight = weights[h : h + 1, :]
        carried_n[:, h, :] = shrink_col[:, h : h + 1] * state_n[:, h, :] + exact_dot(
            across * weight, keys, (1, 0)
        )
        weighted = jnp.concatenate(split(values.T * weight), axis=1)
        key_pair = jnp.concatenate([keys, keys], axis=0).astype(bf16)
        states_in[h].wait()
        for b in range(seqs):
            mask = jnp.where(seq_of_lane == b, 1.0, 0.0).astype(bf16)
            update = jnp.dot(weighted * mask, key_pair, preferred_element_type=f32)
            state_c_v[h, b] = shrink[h : h + 1, b : b + 1] * state_c_v[h, b] + update
        copy = pltpu.make_async_copy(state_c_v.at[h], carried_c.at[:, h], out_sems.at[h])
        copy.start()
        outs.append(copy)
    arrive(outs)


def cell(
    tokens, norm_gain, query_weight, key_weight, value_weight, outgate_weight, gate_weight,
    gate_bias, head_gain, state_c, state_n, state_m, prev_keys, prev_values, prev_gates, accepted,
):
    f32, bf16 = jnp.float32, jnp.bfloat16
    seqs, props, width = tokens.shape
    heads, size = state_n.shape[1:]
    rows, columns = seqs * props, heads * size
    chips = lax.axis_size("kv") // 2
    inputs = (
        accepted,
        tokens,
        norm_gain,
        query_weight,
        key_weight,
        value_weight,
        outgate_weight,
        gate_weight.T,
        gate_bias,
        head_gain,
        state_c,
        state_n,
        state_m.T,
        prev_keys,
        prev_values,
        prev_gates.transpose(1, 2, 3, 0),
    )
    here = pl.BlockSpec(memory_space=pltpu.VMEM)
    anywhere = pl.BlockSpec(memory_space=pl.ANY)
    sent, *fresh = pl.pallas_call(
        cell_kernel,
        out_shape=(
            jax.ShapeDtypeStruct((chips, rows, columns), bf16),
            jax.ShapeDtypeStruct((rows, columns), bf16),
            jax.ShapeDtypeStruct((rows, columns), bf16),
            jax.ShapeDtypeStruct((gate_weight.shape[1], rows), f32),
        ),
        in_specs=[anywhere] * 16,
        out_specs=[anywhere] + [here] * 3,
        scratch_shapes=[
            pltpu.SMEM(accepted.shape, jnp.int32),
            pltpu.VMEM(tokens.shape, bf16),
            pltpu.VMEM((width,), bf16),
            pltpu.VMEM((4, width, columns), bf16),
            pltpu.VMEM(gate_weight.shape[::-1], bf16),
            pltpu.VMEM(gate_bias.shape, f32),
            pltpu.VMEM((columns,), bf16),
            pltpu.VMEM((heads, seqs, size, size), f32),
            pltpu.VMEM(state_n.shape, f32),
            pltpu.VMEM((heads, seqs), f32),
            pltpu.VMEM(prev_keys.shape, bf16),
            pltpu.VMEM(prev_values.shape, bf16),
            pltpu.VMEM((heads, 2, props, seqs), f32),
            pltpu.VMEM((rows, width), f32),
            pltpu.VMEM((rows, width), bf16),
            pltpu.VMEM((rows, columns), f32),
            pltpu.VMEM((rows, columns), f32),
            pltpu.VMEM((rows, columns), bf16),
            pltpu.SemaphoreType.DMA((11 + 16 + heads,)),
            pltpu.SemaphoreType.DMA((chips,)),
        ],
        compiler_params=pltpu.CompilerParams(vmem_limit_bytes=62 * 1024 * 1024),
        cost_estimate=pl.CostEstimate(
            flops=2 * rows * width * 4 * columns, bytes_accessed=22 << 20, transcendentals=0
        ),
    )(*inputs)
    new_c, new_n, new_m, keys, values, gates = pl.pallas_call(
        keep_kernel,
        out_shape=(
            jax.ShapeDtypeStruct(state_c.shape, f32),
            jax.ShapeDtypeStruct(state_n.shape, f32),
            jax.ShapeDtypeStruct((heads, seqs), f32),
            jax.ShapeDtypeStruct(prev_keys.shape, bf16),
            jax.ShapeDtypeStruct(prev_values.shape, bf16),
            jax.ShapeDtypeStruct((heads, 2, props, seqs), f32),
        ),
        in_specs=[pl.BlockSpec(memory_space=pltpu.SMEM), anywhere] + [here] * 8,
        out_specs=[anywhere] + [here] * 5,
        scratch_shapes=[
            pltpu.VMEM((heads, seqs, size, size), f32),
            pltpu.SemaphoreType.DMA((heads,)),
            pltpu.SemaphoreType.DMA((heads,)),
        ],
        compiler_params=pltpu.CompilerParams(vmem_limit_bytes=58 * 1024 * 1024),
        cost_estimate=pl.CostEstimate(
            flops=2 * heads * seqs * size * size * 64, bytes_accessed=9 << 20, transcendentals=0
        ),
    )(accepted, state_c, state_n, inputs[12], prev_keys, prev_values, inputs[15], *fresh)
    return sent, new_c, new_n, new_m.T, keys, values, gates.transpose(3, 0, 1, 2)


def per_device(*arrays):
    inputs, out_weight = arrays[:9] + arrays[10:], arrays[9]
    parts = passed_on(out_weight)
    sent, *rest = cell(*inputs)
    mixed = project_out(sent, parts)
    return (mixed.reshape(-1, inputs[0].shape[1], mixed.shape[1]), *rest)


def solution(mesh):
    in_specs = (
        P("kv", None, None),
        P(),
        P(None, "tp"),
        P(None, "tp"),
        P(None, "tp"),
        P(None, "tp"),
        P(),
        P(),
        P("tp"),
        P("tp", "kv"),
        P("kv", "tp", None, None),
        P("kv", "tp", None),
        P("kv", "tp"),
        P("kv", "tp", None, None),
        P("kv", "tp", None, None),
        P("kv", "tp", None, None),
        P("kv"),
    )
    out_specs = (
        P(None, None, "kv"),
        P("kv", "tp", None, None),
        P("kv", "tp", None),
        P("kv", "tp"),
        P("kv", "tp", None, None),
        P("kv", "tp", None, None),
        P("kv", "tp", None, None),
    )
    return jax.shard_map(
        per_device, mesh=mesh, in_specs=in_specs, out_specs=out_specs, check_vma=False
    )
```

```python
import jax
import jax.numpy as jnp
from jax import lax
from jax.experimental import pallas as pl
from jax.experimental.pallas import tpu as pltpu
from jax.sharding import PartitionSpec as P


EPSILON = 1e-06
HIGHEST = lax.Precision.HIGHEST


def ring(count, step):
    return [(i, (i + step) % count) for i in range(count)]


def swap_cores(x):
    return lax.ppermute(x, "kv", [(i, i ^ 1) for i in range(lax.axis_size("kv"))])


def passed_on(weight):
    tp = lax.axis_size("tp")
    return [weight] + [lax.ppermute(weight, "tp", ring(tp, step)) for step in range(1, tp)]


def mix_kernel(received, *refs):
    weights, out = refs[:-1], refs[-1]
    chips, tp, rows, depth = received.shape
    me = lax.axis_index("tp")
    core = lax.rem(lax.axis_index("kv"), 2)
    total = None
    for step in range(tp):
        source = lax.rem(me - step + tp, tp)
        part = received[:, pl.ds(source, 1)].reshape(chips * rows, depth)
        both = jnp.concatenate([weights[step][...], weights[tp + step][...]], axis=1)
        dot = jnp.dot(part, both, preferred_element_type=jnp.float32)
        total = dot if total is None else total + dot
    mixed = total.astype(jnp.bfloat16)
    columns = mixed.shape[1] // 2
    for x in range(tp):
        out[core, x] = mixed[:, :columns]
        out[1 - core, x] = mixed[:, columns:]


def same_core(kv, tp):
    return [
        [(chip * 2 + core) * tp + x for chip in range(kv // 2) for x in range(tp)]
        for core in (0, 1)
    ]


def same_line(kv, tp):
    return [
        [(chip * 2 + core) * tp + x for core in (0, 1) for x in range(tp)]
        for chip in range(kv // 2)
    ]


def project_out(sent, own_parts):
    kv, tp = lax.axis_size("kv"), lax.axis_size("tp")
    chips = kv // 2
    rows, depth = sent.shape[1] // tp, sent.shape[2]
    other_parts = [swap_cores(part) for part in own_parts]
    received = lax.all_to_all(
        sent.reshape(chips * tp, rows, depth), ("kv", "tp"), 0, 0,
        tiled=True, axis_index_groups=same_core(kv, tp),
    ).reshape(chips, tp, rows, depth)
    columns = own_parts[0].shape[1]
    mixed = pl.pallas_call(
        mix_kernel,
        out_shape=jax.ShapeDtypeStruct((2, tp, chips * rows, columns), jnp.bfloat16),
        compiler_params=pltpu.CompilerParams(vmem_limit_bytes=12 * 1024 * 1024),
        cost_estimate=pl.CostEstimate(
            flops=4 * chips * rows * tp * depth * columns,
            bytes_accessed=3 << 20,
            transcendentals=0,
        ),
    )(received, *own_parts, *other_parts)
    everyone = lax.all_to_all(
        mixed.reshape(2 * tp, chips * rows, columns), ("kv", "tp"), 0, 0,
        tiled=True, axis_index_groups=same_line(kv, tp),
    ).reshape(2, tp, chips, rows, columns)
    return everyone.transpose(2, 0, 1, 3, 4).reshape(-1, columns)


def split(x):
    high = x.astype(jnp.bfloat16)
    return high, (x - high.astype(jnp.float32)).astype(jnp.bfloat16)


def exact_dot(a, b, contract):
    return lax.dot_general(
        a, b, ((contract[:1], contract[1:]), ((), ())),
        precision=HIGHEST, preferred_element_type=jnp.float32,
    )


def dot_nt(a, b):
    return lax.dot_general(
        a, b, (((1,), (1,)), ((), ())), preferred_element_type=jnp.float32
    )


def log_sigmoid(x):
    return jnp.minimum(x, 0.0) - jnp.log1p(jnp.exp(-jnp.abs(x)))


def iota(shape, dim):
    return lax.broadcasted_iota(jnp.int32, shape, dim)


def bringer(sems):
    copies = []

    def bring(src, dst):
        copy = pltpu.make_async_copy(src, dst, sems.at[len(copies)])
        copies.append(copy)
        copy.start()
        return copy

    return bring


def arrive(some):
    for copy in some:
        copy.wait()


def spreads(seqs, rows):
    across = jnp.where(iota((seqs, rows), 0) == (iota((seqs, rows), 1) >> 2), 1.0, 0.0)
    down = jnp.where((iota((rows, seqs), 0) >> 2) == iota((rows, seqs), 1), 1.0, 0.0)
    return across, down


def replay(accepted, state_m, prev_gates, across):
    heads, _, props, seqs = prev_gates.shape
    seq_lane = iota((1, seqs), 1)
    counts = jnp.zeros((1, seqs), jnp.int32)
    for b in range(seqs):
        counts = jnp.where(seq_lane == b, accepted[b], counts)
    total = jnp.zeros((heads, seqs), jnp.float32)
    sums, inputs = [], []
    for s in range(props):
        both = [
            jnp.concatenate([prev_gates[h, g, s : s + 1, :] for h in range(heads)], axis=0)
            for g in (0, 1)
        ]
        total = total + jnp.where(counts > s, log_sigmoid(both[1]), 0.0)
        sums.append(total)
        inputs.append(both[0])
    logs = [
        jnp.where(counts > s, total - sums[s] + inputs[s], -jnp.inf) for s in range(props)
    ]
    decayed = total + state_m[...]
    stable = decayed
    for s in range(props):
        stable = jnp.maximum(stable, logs[s])
    shrink = jnp.exp(decayed - stable)
    prop_lane = iota((1, across.shape[1]), 1) & (props - 1)
    weights = jnp.zeros((heads, across.shape[1]), jnp.float32)
    for s in range(props):
        spaced = exact_dot(jnp.exp(logs[s] - stable), across, (1, 0))
        weights = weights + jnp.where(prop_lane == s, spaced, 0.0)
    return stable, shrink, weights


def cell_kernel(
    accepted,
    tokens,
    norm_gain,
    query_weight,
    key_weight,
    value_weight,
    outgate_weight,
    gate_weight,
    gate_bias,
    head_gain,
    state_c,
    state_n,
    state_m,
    prev_keys,
    prev_values,
    prev_gates,
    gated_out,
    keys_out,
    values_out,
    gates_out,
    accepted_s,
    tokens_v,
    gain_v,
    weights_v,
    gate_weight_v,
    gate_bias_v,
    head_gain_v,
    state_c_v,
    state_n_v,
    state_m_v,
    prev_keys_v,
    prev_values_v,
    prev_gates_v,
    normed_f,
    normed_v,
    recall_v,
    hidden_v,
    gated_v,
    keys_v,
    values_v,
    gates_v,
    sems,
    out_sems,
):
    f32, bf16 = jnp.float32, jnp.bfloat16
    seqs, props, width = tokens_v.shape
    heads, _, size, _ = state_c_v.shape
    rows = seqs * props
    heads_total = gate_weight_v.shape[0] // 2
    scale = size ** (-0.5)
    pieces = 4
    depth = width // pieces
    bring = bringer(sems)

    def bring_weight(which, src):
        return [
            bring(src.at[pl.ds(p * depth, depth)], weights_v.at[which, pl.ds(p * depth, depth)])
            for p in range(pieces)
        ]

    early = [bring(tokens, tokens_v), bring(norm_gain, gain_v)]
    gates_in = [bring(gate_weight, gate_weight_v), bring(gate_bias, gate_bias_v)]
    replay_in = [
        bring(accepted, accepted_s),
        bring(state_m, state_m_v),
        bring(prev_gates, prev_gates_v),
        bring(state_n, state_n_v),
        bring(prev_keys, prev_keys_v),
        bring(prev_values, prev_values_v),
        bring(head_gain, head_gain_v),
    ]
    weights_in = [bring_weight(0, query_weight)]
    states_in = [bring(state_c.at[:, h], state_c_v.at[h]) for h in range(heads)]
    weights_in += [
        bring_weight(1, key_weight),
        bring_weight(2, value_weight),
        bring_weight(3, outgate_weight),
    ]

    across, down = spreads(seqs, rows)
    square = (rows, rows)
    same = (iota(square, 0) >> 2) == (iota(square, 1) >> 2)
    causal = same & (iota(square, 0) >= iota(square, 1))

    arrive(early)
    gain = gain_v[...].astype(f32).reshape(1, width)
    for b in range(seqs):
        x = tokens_v[b].astype(f32)
        mean = jnp.mean(x * x, axis=-1, keepdims=True)
        normed_f[b * props : (b + 1) * props, :] = x * lax.rsqrt(mean + EPSILON) * gain
    normed_v[...] = normed_f[...].astype(bf16)

    arrive(gates_in)
    bias = jnp.concatenate([gate_bias_v[0:1, :], gate_bias_v[1:2, :]], axis=1)
    gates = dot_nt(normed_v[...], gate_weight_v[...]) + bias
    gates = jnp.concatenate([gates, jnp.zeros((rows, 128 - 2 * heads_total), f32)], axis=1)
    first_head = lax.axis_index("tp") * heads
    gates = pltpu.roll(gates, 128 - first_head, 1)
    cumul = exact_dot(jnp.where(causal, 1.0, 0.0), log_sigmoid(gates), (1, 0))
    gates_t = gates.T
    cumul_t = cumul.T
    gates_v[...] = gates_t[: 2 * heads_total]
    sends = [pltpu.make_async_copy(gates_v, gates_out, out_sems.at[0])]
    sends[0].start()

    arrive(replay_in)
    stable, shrink, weights = replay(accepted_s, state_m_v, prev_gates_v, across)
    weights = weights * scale
    stable_col = exact_dot(down, stable, (1, 1))
    shrink_col = exact_dot(down, shrink, (1, 1))

    def project(which):
        acc = None
        for p in range(pieces):
            weights_in[which][p].wait()
            part = jnp.dot(
                normed_v[:, p * depth : (p + 1) * depth],
                weights_v[which, p * depth : (p + 1) * depth, :],
                preferred_element_type=f32,
            )
            acc = part if acc is None else acc + part
        return acc.astype(bf16)

    queries = project(0)
    upper = iota((2 * props, size), 0) < props
    for h in range(heads):
        cols = slice(h * size, (h + 1) * size)
        query_f = queries[:, cols].astype(f32)
        states_in[h].wait()
        for p in range(seqs // 2):
            stacked = [
                jnp.concatenate(split(state_c_v[h, b]), axis=1) for b in (2 * p, 2 * p + 1)
            ]
            pair = slice(2 * p * props, 2 * (p + 1) * props)
            asked = query_f[pair].astype(bf16)
            found = dot_nt(
                jnp.concatenate([asked, asked], axis=1), jnp.concatenate(stacked, axis=0)
            )
            recall_v[pair, cols] = jnp.where(upper, found[:, :size], found[:, size:])

    new_keys = project(1)
    keys_v[...] = new_keys
    sends.append(pltpu.make_async_copy(keys_v, keys_out, out_sems.at[1]))
    sends[1].start()
    new_values = project(2)
    values_v[...] = new_values
    sends.append(pltpu.make_async_copy(values_v, values_out, out_sems.at[2]))
    sends[2].start()
    for h in range(heads):
        cols = slice(h * size, (h + 1) * size)
        query, key, value = queries[:, cols], new_keys[:, cols], new_values[:, cols]
        old_key = prev_keys_v[:, h].astype(f32).reshape(rows, size).astype(bf16)
        old_value = prev_values_v[:, h].astype(f32).reshape(rows, size).astype(bf16)
        c_col = cumul[:, heads_total + h : heads_total + h + 1]
        c_row = cumul_t[heads_total + h : heads_total + h + 1, :]
        i_row = gates_t[h : h + 1, :]
        logs_ts = jnp.where(causal, c_col - c_row + i_row, -jnp.inf)
        carried = c_col + stable_col[:, h : h + 1]
        steady = jnp.maximum(carried, jnp.max(logs_ts, axis=1, keepdims=True))
        weight_state = jnp.exp(carried - steady)
        scores = dot_nt(query, key) * scale * jnp.exp(logs_ts - steady)
        replayed = jnp.where(same, dot_nt(query, old_key) * weights[h : h + 1, :], 0.0)
        both = jnp.concatenate([weight_state * replayed, scores], axis=1)
        kept = weight_state * shrink_col[:, h : h + 1]
        numer = kept * recall_v[:, cols] + jnp.dot(
            jnp.concatenate(split(both), axis=1),
            jnp.concatenate([old_value, value] * 2, axis=0),
            preferred_element_type=f32,
        )
        along = exact_dot(query.astype(f32), state_n_v[:, h, :], (1, 1))
        recall_norm = jnp.sum(along * down, axis=1, keepdims=True)
        denom = kept * recall_norm + jnp.sum(both, axis=1, keepdims=True)
        hidden = numer / jnp.maximum(jnp.abs(denom), jnp.exp(-steady))
        hidden_v[:, cols] = hidden * lax.rsqrt(
            jnp.mean(hidden * hidden, axis=1, keepdims=True) + EPSILON
        )

    outgate = project(3)
    head_scale = head_gain_v[...].astype(f32).reshape(1, heads * size)
    gated_v[...] = (
        hidden_v[...] * head_scale * jax.nn.sigmoid(outgate.astype(f32))
    ).astype(bf16)
    for chip in range(gated_out.shape[0]):
        copy = pltpu.make_async_copy(gated_v, gated_out.at[chip], out_sems.at[3 + chip])
        copy.start()
        sends.append(copy)
    arrive(sends)


def keep_kernel(
    accepted,
    state_c,
    state_n,
    state_m,
    prev_keys,
    prev_values,
    prev_gates,
    new_keys,
    new_values,
    gates_t,
    carried_c,
    carried_n,
    carried_m,
    step_keys,
    step_values,
    step_gates,
    state_c_v,
    sems,
    out_sems,
):
    f32, bf16 = jnp.float32, jnp.bfloat16
    heads, seqs, size, _ = state_c_v.shape
    props = prev_gates.shape[2]
    rows = seqs * props
    scale = size ** (-0.5)
    bring = bringer(sems)
    states_in = [bring(state_c.at[:, h], state_c_v.at[h]) for h in range(heads)]
    across, _ = spreads(seqs, rows)
    for t in range(props):
        pick = jnp.where(iota((rows, seqs), 0) == iota((rows, seqs), 1) * props + t, 1.0, 0.0)
        picked = exact_dot(gates_t[...], pick, (1, 0))
        total = picked.shape[0] // 2
        for h in range(heads):
            step_gates[h, 0, t : t + 1, :] = picked[h : h + 1, :]
            step_gates[h, 1, t : t + 1, :] = picked[total + h : total + h + 1, :]
    stable, shrink, weights = replay(accepted, state_m, prev_gates, across)
    weights = weights * scale
    carried_m[...] = stable
    diagonal = jnp.where(iota((seqs, seqs), 0) == iota((seqs, seqs), 1), 1.0, 0.0)
    shrink_col = exact_dot(diagonal, shrink, (1, 1))
    seq_of_lane = (iota((1, 2 * rows), 1) & (rows - 1)) >> 2
    outs = []
    for h in range(heads):
        cols = slice(h * size, (h + 1) * size)
        step_keys[:, h] = new_keys[:, cols].astype(f32).reshape(seqs, props, size).astype(bf16)
        step_values[:, h] = new_values[:, cols].astype(f32).reshape(seqs, props, size).astype(bf16)
        keys = prev_keys[:, h].astype(f32).reshape(rows, size)
        values = prev_values[:, h].astype(f32).reshape(rows, size)
        weight = weights[h : h + 1, :]
        carried_n[:, h, :] = shrink_col[:, h : h + 1] * state_n[:, h, :] + exact_dot(
            across * weight, keys, (1, 0)
        )
        weighted = jnp.concatenate(split(values.T * weight), axis=1)
        key_pair = jnp.concatenate([keys, keys], axis=0).astype(bf16)
        states_in[h].wait()
        for b in range(seqs):
            mask = jnp.where(seq_of_lane == b, 1.0, 0.0).astype(bf16)
            update = jnp.dot(weighted * mask, key_pair, preferred_element_type=f32)
            state_c_v[h, b] = shrink[h : h + 1, b : b + 1] * state_c_v[h, b] + update
        copy = pltpu.make_async_copy(state_c_v.at[h], carried_c.at[:, h], out_sems.at[h])
        copy.start()
        outs.append(copy)
    arrive(outs)


def cell(
    tokens, norm_gain, query_weight, key_weight, value_weight, outgate_weight, gate_weight,
    gate_bias, head_gain, state_c, state_n, state_m, prev_keys, prev_values, prev_gates, accepted,
):
    f32, bf16 = jnp.float32, jnp.bfloat16
    seqs, props, width = tokens.shape
    heads, size = state_n.shape[1:]
    rows, columns = seqs * props, heads * size
    chips = lax.axis_size("kv") // 2
    inputs = (
        accepted,
        tokens,
        norm_gain,
        query_weight,
        key_weight,
        value_weight,
        outgate_weight,
        gate_weight.T,
        gate_bias,
        head_gain,
        state_c,
        state_n,
        state_m.T,
        prev_keys,
        prev_values,
        prev_gates.transpose(1, 2, 3, 0),
    )
    here = pl.BlockSpec(memory_space=pltpu.VMEM)
    anywhere = pl.BlockSpec(memory_space=pl.ANY)
    sent, *fresh = pl.pallas_call(
        cell_kernel,
        out_shape=(
            jax.ShapeDtypeStruct((chips, rows, columns), bf16),
            jax.ShapeDtypeStruct((rows, columns), bf16),
            jax.ShapeDtypeStruct((rows, columns), bf16),
            jax.ShapeDtypeStruct((gate_weight.shape[1], rows), f32),
        ),
        in_specs=[anywhere] * 16,
        out_specs=[anywhere] * 4,
        scratch_shapes=[
            pltpu.SMEM(accepted.shape, jnp.int32),
            pltpu.VMEM(tokens.shape, bf16),
            pltpu.VMEM((width,), bf16),
            pltpu.VMEM((4, width, columns), bf16),
            pltpu.VMEM(gate_weight.shape[::-1], bf16),
            pltpu.VMEM(gate_bias.shape, f32),
            pltpu.VMEM((columns,), bf16),
            pltpu.VMEM((heads, seqs, size, size), f32),
            pltpu.VMEM(state_n.shape, f32),
            pltpu.VMEM((heads, seqs), f32),
            pltpu.VMEM(prev_keys.shape, bf16),
            pltpu.VMEM(prev_values.shape, bf16),
            pltpu.VMEM((heads, 2, props, seqs), f32),
            pltpu.VMEM((rows, width), f32),
            pltpu.VMEM((rows, width), bf16),
            pltpu.VMEM((rows, columns), f32),
            pltpu.VMEM((rows, columns), f32),
            pltpu.VMEM((rows, columns), bf16),
            pltpu.VMEM((rows, columns), bf16),
            pltpu.VMEM((rows, columns), bf16),
            pltpu.VMEM((gate_weight.shape[1], rows), f32),
            pltpu.SemaphoreType.DMA((11 + 16 + heads,)),
            pltpu.SemaphoreType.DMA((3 + chips,)),
        ],
        compiler_params=pltpu.CompilerParams(vmem_limit_bytes=62 * 1024 * 1024),
        cost_estimate=pl.CostEstimate(
            flops=2 * rows * width * 4 * columns, bytes_accessed=22 << 20, transcendentals=0
        ),
    )(*inputs)
    new_c, new_n, new_m, keys, values, gates = pl.pallas_call(
        keep_kernel,
        out_shape=(
            jax.ShapeDtypeStruct(state_c.shape, f32),
            jax.ShapeDtypeStruct(state_n.shape, f32),
            jax.ShapeDtypeStruct((heads, seqs), f32),
            jax.ShapeDtypeStruct(prev_keys.shape, bf16),
            jax.ShapeDtypeStruct(prev_values.shape, bf16),
            jax.ShapeDtypeStruct((heads, 2, props, seqs), f32),
        ),
        in_specs=[pl.BlockSpec(memory_space=pltpu.SMEM), anywhere] + [here] * 8,
        out_specs=[anywhere] + [here] * 5,
        scratch_shapes=[
            pltpu.VMEM((heads, seqs, size, size), f32),
            pltpu.SemaphoreType.DMA((heads,)),
            pltpu.SemaphoreType.DMA((heads,)),
        ],
        compiler_params=pltpu.CompilerParams(vmem_limit_bytes=58 * 1024 * 1024),
        cost_estimate=pl.CostEstimate(
            flops=2 * heads * seqs * size * size * 64, bytes_accessed=9 << 20, transcendentals=0
        ),
    )(accepted, state_c, state_n, inputs[12], prev_keys, prev_values, inputs[15], *fresh)
    return sent, new_c, new_n, new_m.T, keys, values, gates.transpose(3, 0, 1, 2)


def per_device(*arrays):
    inputs, out_weight = arrays[:9] + arrays[10:], arrays[9]
    parts = passed_on(out_weight)
    sent, *rest = cell(*inputs)
    mixed = project_out(sent, parts)
    return (mixed.reshape(-1, inputs[0].shape[1], mixed.shape[1]), *rest)


def solution(mesh):
    in_specs = (
        P("kv", None, None),
        P(),
        P(None, "tp"),
        P(None, "tp"),
        P(None, "tp"),
        P(None, "tp"),
        P(),
        P(),
        P("tp"),
        P("tp", "kv"),
        P("kv", "tp", None, None),
        P("kv", "tp", None),
        P("kv", "tp"),
        P("kv", "tp", None, None),
        P("kv", "tp", None, None),
        P("kv", "tp", None, None),
        P("kv"),
    )
    out_specs = (
        P(None, None, "kv"),
        P("kv", "tp", None, None),
        P("kv", "tp", None),
        P("kv", "tp"),
        P("kv", "tp", None, None),
        P("kv", "tp", None, None),
        P("kv", "tp", None, None),
    )
    return jax.shard_map(
        per_device, mesh=mesh, in_specs=in_specs, out_specs=out_specs, check_vma=False
    )
```

```python
import jax
import jax.numpy as jnp
from jax import lax
from jax.experimental import pallas as pl
from jax.experimental.pallas import tpu as pltpu
from jax.sharding import PartitionSpec as P


EPSILON = 1e-06
HIGHEST = lax.Precision.HIGHEST


def ring(count, step):
    return [(i, (i + step) % count) for i in range(count)]


def swap_cores(x):
    return lax.ppermute(x, "kv", [(i, i ^ 1) for i in range(lax.axis_size("kv"))])


def passed_on(weight):
    tp = lax.axis_size("tp")
    passed = [weight]
    for step in range(1, tp):
        passed.append(lax.ppermute(weight, "tp", ring(tp, step)))
    return passed


def mix_kernel(received, *refs):
    weights, out = refs[:-1], refs[-1]
    chips, tp, rows, depth = received.shape
    me = lax.axis_index("tp")
    core = lax.rem(lax.axis_index("kv"), 2)
    total = None
    for step in range(tp):
        source = lax.rem(me - step + tp, tp)
        part = received[:, pl.ds(source, 1)].reshape(chips * rows, depth)
        both = jnp.concatenate([weights[step][...], weights[tp + step][...]], axis=1)
        dot = jnp.dot(part, both, preferred_element_type=jnp.float32)
        total = dot if total is None else total + dot
    mixed = total.astype(jnp.bfloat16)
    columns = mixed.shape[1] // 2
    for x in range(tp):
        out[core, x] = mixed[:, :columns]
        out[1 - core, x] = mixed[:, columns:]


def same_core(kv, tp):
    return [
        [(chip * 2 + core) * tp + x for chip in range(kv // 2) for x in range(tp)]
        for core in (0, 1)
    ]


def same_line(kv, tp):
    return [
        [(chip * 2 + core) * tp + x for core in (0, 1) for x in range(tp)]
        for chip in range(kv // 2)
    ]


def project_out(sent, own_parts):
    kv, tp = lax.axis_size("kv"), lax.axis_size("tp")
    chips = kv // 2
    rows, depth = sent.shape[1] // tp, sent.shape[2]
    other_parts = [swap_cores(part) for part in own_parts]
    received = lax.all_to_all(
        sent.reshape(chips * tp, rows, depth), ("kv", "tp"), 0, 0,
        tiled=True, axis_index_groups=same_core(kv, tp),
    ).reshape(chips, tp, rows, depth)
    columns = own_parts[0].shape[1]
    mixed = pl.pallas_call(
        mix_kernel,
        out_shape=jax.ShapeDtypeStruct((2, tp, chips * rows, columns), jnp.bfloat16),
        compiler_params=pltpu.CompilerParams(vmem_limit_bytes=12 * 1024 * 1024),
        cost_estimate=pl.CostEstimate(
            flops=4 * chips * rows * tp * depth * columns,
            bytes_accessed=3 << 20,
            transcendentals=0,
        ),
    )(received, *own_parts, *other_parts)
    everyone = lax.all_to_all(
        mixed.reshape(2 * tp, chips * rows, columns), ("kv", "tp"), 0, 0,
        tiled=True, axis_index_groups=same_line(kv, tp),
    ).reshape(2, tp, chips, rows, columns)
    return everyone.transpose(2, 0, 1, 3, 4).reshape(-1, columns)


def split(x):
    high = x.astype(jnp.bfloat16)
    return high, (x - high.astype(jnp.float32)).astype(jnp.bfloat16)


def exact_dot(a, b, contract):
    return lax.dot_general(
        a, b, ((contract[:1], contract[1:]), ((), ())),
        precision=HIGHEST, preferred_element_type=jnp.float32,
    )


def dot_nt(a, b):
    return lax.dot_general(
        a, b, (((1,), (1,)), ((), ())), preferred_element_type=jnp.float32
    )


def log_sigmoid(x):
    return jnp.minimum(x, 0.0) - jnp.log1p(jnp.exp(-jnp.abs(x)))


def iota(shape, dim):
    return lax.broadcasted_iota(jnp.int32, shape, dim)


def bringer(sems):
    copies = []

    def bring(src, dst):
        copy = pltpu.make_async_copy(src, dst, sems.at[len(copies)])
        copies.append(copy)
        copy.start()
        return copy

    return bring


def arrive(some):
    for copy in some:
        copy.wait()


def spreads(seqs, rows):
    across = jnp.where(iota((seqs, rows), 0) == (iota((seqs, rows), 1) >> 2), 1.0, 0.0)
    down = jnp.where((iota((rows, seqs), 0) >> 2) == iota((rows, seqs), 1), 1.0, 0.0)
    return across, down


def replay(accepted, state_m, prev_gates, across):
    heads, _, props, seqs = prev_gates.shape
    seq_lane = iota((1, seqs), 1)
    counts = jnp.zeros((1, seqs), jnp.int32)
    for b in range(seqs):
        counts = jnp.where(seq_lane == b, accepted[b], counts)
    total = jnp.zeros((heads, seqs), jnp.float32)
    sums, inputs = [], []
    for s in range(props):
        both = [
            jnp.concatenate([prev_gates[h, g, s : s + 1, :] for h in range(heads)], axis=0)
            for g in (0, 1)
        ]
        total = total + jnp.where(counts > s, log_sigmoid(both[1]), 0.0)
        sums.append(total)
        inputs.append(both[0])
    logs = [
        jnp.where(counts > s, total - sums[s] + inputs[s], -jnp.inf) for s in range(props)
    ]
    decayed = total + state_m[...]
    stable = decayed
    for s in range(props):
        stable = jnp.maximum(stable, logs[s])
    shrink = jnp.exp(decayed - stable)
    prop_lane = iota((1, across.shape[1]), 1) & (props - 1)
    weights = jnp.zeros((heads, across.shape[1]), jnp.float32)
    for s in range(props):
        spaced = exact_dot(jnp.exp(logs[s] - stable), across, (1, 0))
        weights = weights + jnp.where(prop_lane == s, spaced, 0.0)
    return stable, shrink, weights


def cell_kernel(
    accepted,
    tokens,
    norm_gain,
    query_weight,
    key_weight,
    value_weight,
    outgate_weight,
    gate_weight,
    gate_bias,
    head_gain,
    state_c,
    state_n,
    state_m,
    prev_keys,
    prev_values,
    prev_gates,
    gated_out,
    keys_out,
    values_out,
    gates_out,
    accepted_s,
    tokens_v,
    gain_v,
    weights_v,
    gate_weight_v,
    gate_bias_v,
    head_gain_v,
    state_c_v,
    state_n_v,
    state_m_v,
    prev_keys_v,
    prev_values_v,
    prev_gates_v,
    normed_f,
    normed_v,
    recall_v,
    hidden_v,
    gated_v,
    keys_v,
    values_v,
    gates_v,
    sems,
    out_sems,
):
    f32, bf16 = jnp.float32, jnp.bfloat16
    seqs, props, width = tokens_v.shape
    heads, _, size, _ = state_c_v.shape
    rows = seqs * props
    heads_total = gate_weight_v.shape[0] // 2
    scale = size ** (-0.5)
    pieces = 4
    depth = width // pieces
    bring = bringer(sems)

    def bring_weight(which, src):
        return [
            bring(src.at[pl.ds(p * depth, depth)], weights_v.at[which, pl.ds(p * depth, depth)])
            for p in range(pieces)
        ]

    early = [bring(tokens, tokens_v), bring(norm_gain, gain_v)]
    gates_in = [bring(gate_weight, gate_weight_v), bring(gate_bias, gate_bias_v)]
    replay_in = [
        bring(accepted, accepted_s),
        bring(state_m, state_m_v),
        bring(prev_gates, prev_gates_v),
        bring(state_n, state_n_v),
        bring(prev_keys, prev_keys_v),
        bring(prev_values, prev_values_v),
        bring(head_gain, head_gain_v),
    ]
    weights_in = [bring_weight(0, query_weight)]
    states_in = [bring(state_c.at[:, h], state_c_v.at[h]) for h in range(heads)]
    weights_in += [
        bring_weight(1, key_weight),
        bring_weight(2, value_weight),
        bring_weight(3, outgate_weight),
    ]

    across, down = spreads(seqs, rows)
    square = (rows, rows)
    same = (iota(square, 0) >> 2) == (iota(square, 1) >> 2)
    causal = same & (iota(square, 0) >= iota(square, 1))

    arrive(early)
    gain = gain_v[...].astype(f32).reshape(1, width)
    for b in range(seqs):
        x = tokens_v[b].astype(f32)
        mean = jnp.mean(x * x, axis=-1, keepdims=True)
        normed_f[b * props : (b + 1) * props, :] = x * lax.rsqrt(mean + EPSILON) * gain
    normed_v[...] = normed_f[...].astype(bf16)

    arrive(gates_in)
    bias = jnp.concatenate([gate_bias_v[0:1, :], gate_bias_v[1:2, :]], axis=1)
    gates = dot_nt(normed_v[...], gate_weight_v[...]) + bias
    gates = jnp.concatenate([gates, jnp.zeros((rows, 128 - 2 * heads_total), f32)], axis=1)
    first_head = lax.axis_index("tp") * heads
    gates = pltpu.roll(gates, 128 - first_head, 1)
    cumul = exact_dot(jnp.where(causal, 1.0, 0.0), log_sigmoid(gates), (1, 0))
    gates_t = gates.T
    cumul_t = cumul.T
    gates_v[...] = gates_t[: 2 * heads_total]
    sends = [pltpu.make_async_copy(gates_v, gates_out, out_sems.at[0])]
    sends[0].start()

    arrive(replay_in)
    stable, shrink, weights = replay(accepted_s, state_m_v, prev_gates_v, across)
    weights = weights * scale
    stable_col = exact_dot(down, stable, (1, 1))
    shrink_col = exact_dot(down, shrink, (1, 1))

    def project(which):
        acc = None
        for p in range(pieces):
            weights_in[which][p].wait()
            part = jnp.dot(
                normed_v[:, p * depth : (p + 1) * depth],
                weights_v[which, p * depth : (p + 1) * depth, :],
                preferred_element_type=f32,
            )
            acc = part if acc is None else acc + part
        return acc.astype(bf16)

    queries = project(0)
    upper = iota((2 * props, size), 0) < props
    for h in range(heads):
        cols = slice(h * size, (h + 1) * size)
        query_f = queries[:, cols].astype(f32)
        states_in[h].wait()
        for p in range(seqs // 2):
            stacked = [
                jnp.concatenate(split(state_c_v[h, b]), axis=1) for b in (2 * p, 2 * p + 1)
            ]
            pair = slice(2 * p * props, 2 * (p + 1) * props)
            asked = query_f[pair].astype(bf16)
            found = dot_nt(
                jnp.concatenate([asked, asked], axis=1), jnp.concatenate(stacked, axis=0)
            )
            recall_v[pair, cols] = jnp.where(upper, found[:, :size], found[:, size:])

    new_keys = project(1)
    keys_v[...] = new_keys
    sends.append(pltpu.make_async_copy(keys_v, keys_out, out_sems.at[1]))
    sends[1].start()
    new_values = project(2)
    values_v[...] = new_values
    sends.append(pltpu.make_async_copy(values_v, values_out, out_sems.at[2]))
    sends[2].start()
    for h in range(heads):
        cols = slice(h * size, (h + 1) * size)
        query, key, value = queries[:, cols], new_keys[:, cols], new_values[:, cols]
        old_key = prev_keys_v[:, h].astype(f32).reshape(rows, size).astype(bf16)
        old_value = prev_values_v[:, h].astype(f32).reshape(rows, size).astype(bf16)
        c_col = cumul[:, heads_total + h : heads_total + h + 1]
        c_row = cumul_t[heads_total + h : heads_total + h + 1, :]
        i_row = gates_t[h : h + 1, :]
        logs_ts = jnp.where(causal, c_col - c_row + i_row, -jnp.inf)
        carried = c_col + stable_col[:, h : h + 1]
        steady = jnp.maximum(carried, jnp.max(logs_ts, axis=1, keepdims=True))
        weight_state = jnp.exp(carried - steady)
        scores = dot_nt(query, key) * scale * jnp.exp(logs_ts - steady)
        replayed = jnp.where(same, dot_nt(query, old_key) * weights[h : h + 1, :], 0.0)
        both = jnp.concatenate([weight_state * replayed, scores], axis=1)
        kept = weight_state * shrink_col[:, h : h + 1]
        numer = kept * recall_v[:, cols] + jnp.dot(
            jnp.concatenate(split(both), axis=1),
            jnp.concatenate([old_value, value] * 2, axis=0),
            preferred_element_type=f32,
        )
        along = exact_dot(query.astype(f32), state_n_v[:, h, :], (1, 1))
        recall_norm = jnp.sum(along * down, axis=1, keepdims=True)
        denom = kept * recall_norm + jnp.sum(both, axis=1, keepdims=True)
        hidden = numer / jnp.maximum(jnp.abs(denom), jnp.exp(-steady))
        hidden_v[:, cols] = hidden * lax.rsqrt(
            jnp.mean(hidden * hidden, axis=1, keepdims=True) + EPSILON
        )

    outgate = project(3)
    head_scale = head_gain_v[...].astype(f32).reshape(1, heads * size)
    gated_v[...] = (
        hidden_v[...] * head_scale * jax.nn.sigmoid(outgate.astype(f32))
    ).astype(bf16)
    for chip in range(gated_out.shape[0]):
        copy = pltpu.make_async_copy(gated_v, gated_out.at[chip], out_sems.at[3 + chip])
        copy.start()
        sends.append(copy)
    arrive(sends)


def keep_kernel(
    accepted,
    state_c,
    state_n,
    state_m,
    prev_keys,
    prev_values,
    prev_gates,
    new_keys,
    new_values,
    gates_t,
    carried_c,
    carried_n,
    carried_m,
    step_keys,
    step_values,
    step_gates,
    state_c_v,
    sems,
    out_sems,
):
    f32, bf16 = jnp.float32, jnp.bfloat16
    heads, seqs, size, _ = state_c_v.shape
    props = prev_gates.shape[2]
    rows = seqs * props
    scale = size ** (-0.5)
    bring = bringer(sems)
    states_in = [bring(state_c.at[:, h], state_c_v.at[h]) for h in range(heads)]
    across, _ = spreads(seqs, rows)
    for t in range(props):
        pick = jnp.where(iota((rows, seqs), 0) == iota((rows, seqs), 1) * props + t, 1.0, 0.0)
        picked = exact_dot(gates_t[...], pick, (1, 0))
        total = picked.shape[0] // 2
        for h in range(heads):
            step_gates[h, 0, t : t + 1, :] = picked[h : h + 1, :]
            step_gates[h, 1, t : t + 1, :] = picked[total + h : total + h + 1, :]
    stable, shrink, weights = replay(accepted, state_m, prev_gates, across)
    weights = weights * scale
    carried_m[...] = stable
    diagonal = jnp.where(iota((seqs, seqs), 0) == iota((seqs, seqs), 1), 1.0, 0.0)
    shrink_col = exact_dot(diagonal, shrink, (1, 1))
    seq_of_lane = (iota((1, 2 * rows), 1) & (rows - 1)) >> 2
    outs = []
    for h in range(heads):
        cols = slice(h * size, (h + 1) * size)
        step_keys[:, h] = new_keys[:, cols].astype(f32).reshape(seqs, props, size).astype(bf16)
        step_values[:, h] = new_values[:, cols].astype(f32).reshape(seqs, props, size).astype(bf16)
        keys = prev_keys[:, h].astype(f32).reshape(rows, size)
        values = prev_values[:, h].astype(f32).reshape(rows, size)
        weight = weights[h : h + 1, :]
        carried_n[:, h, :] = shrink_col[:, h : h + 1] * state_n[:, h, :] + exact_dot(
            across * weight, keys, (1, 0)
        )
        weighted = jnp.concatenate(split(values.T * weight), axis=1)
        key_pair = jnp.concatenate([keys, keys], axis=0).astype(bf16)
        states_in[h].wait()
        for b in range(seqs):
            mask = jnp.where(seq_of_lane == b, 1.0, 0.0).astype(bf16)
            update = jnp.dot(weighted * mask, key_pair, preferred_element_type=f32)
            state_c_v[h, b] = shrink[h : h + 1, b : b + 1] * state_c_v[h, b] + update
        copy = pltpu.make_async_copy(state_c_v.at[h], carried_c.at[:, h], out_sems.at[h])
        copy.start()
        outs.append(copy)
    arrive(outs)


def cell(
    tokens, norm_gain, query_weight, key_weight, value_weight, outgate_weight, gate_weight,
    gate_bias, head_gain, state_c, state_n, state_m, prev_keys, prev_values, prev_gates, accepted,
):
    f32, bf16 = jnp.float32, jnp.bfloat16
    seqs, props, width = tokens.shape
    heads, size = state_n.shape[1:]
    rows, columns = seqs * props, heads * size
    chips = lax.axis_size("kv") // 2
    inputs = (
        accepted,
        tokens,
        norm_gain,
        query_weight,
        key_weight,
        value_weight,
        outgate_weight,
        gate_weight.T,
        gate_bias,
        head_gain,
        state_c,
        state_n,
        state_m.T,
        prev_keys,
        prev_values,
        prev_gates.transpose(1, 2, 3, 0),
    )
    here = pl.BlockSpec(memory_space=pltpu.VMEM)
    anywhere = pl.BlockSpec(memory_space=pl.ANY)
    sent, *fresh = pl.pallas_call(
        cell_kernel,
        out_shape=(
            jax.ShapeDtypeStruct((chips, rows, columns), bf16),
            jax.ShapeDtypeStruct((rows, columns), bf16),
            jax.ShapeDtypeStruct((rows, columns), bf16),
            jax.ShapeDtypeStruct((gate_weight.shape[1], rows), f32),
        ),
        in_specs=[anywhere] * 16,
        out_specs=[anywhere] * 4,
        scratch_shapes=[
            pltpu.SMEM(accepted.shape, jnp.int32),
            pltpu.VMEM(tokens.shape, bf16),
            pltpu.VMEM((width,), bf16),
            pltpu.VMEM((4, width, columns), bf16),
            pltpu.VMEM(gate_weight.shape[::-1], bf16),
            pltpu.VMEM(gate_bias.shape, f32),
            pltpu.VMEM((columns,), bf16),
            pltpu.VMEM((heads, seqs, size, size), f32),
            pltpu.VMEM(state_n.shape, f32),
            pltpu.VMEM((heads, seqs), f32),
            pltpu.VMEM(prev_keys.shape, bf16),
            pltpu.VMEM(prev_values.shape, bf16),
            pltpu.VMEM((heads, 2, props, seqs), f32),
            pltpu.VMEM((rows, width), f32),
            pltpu.VMEM((rows, width), bf16),
            pltpu.VMEM((rows, columns), f32),
            pltpu.VMEM((rows, columns), f32),
            pltpu.VMEM((rows, columns), bf16),
            pltpu.VMEM((rows, columns), bf16),
            pltpu.VMEM((rows, columns), bf16),
            pltpu.VMEM((gate_weight.shape[1], rows), f32),
            pltpu.SemaphoreType.DMA((11 + 16 + heads,)),
            pltpu.SemaphoreType.DMA((3 + chips,)),
        ],
        compiler_params=pltpu.CompilerParams(vmem_limit_bytes=62 * 1024 * 1024),
        cost_estimate=pl.CostEstimate(
            flops=2 * rows * width * 4 * columns, bytes_accessed=22 << 20, transcendentals=0
        ),
    )(*inputs)
    new_c, new_n, new_m, keys, values, gates = pl.pallas_call(
        keep_kernel,
        out_shape=(
            jax.ShapeDtypeStruct(state_c.shape, f32),
            jax.ShapeDtypeStruct(state_n.shape, f32),
            jax.ShapeDtypeStruct((heads, seqs), f32),
            jax.ShapeDtypeStruct(prev_keys.shape, bf16),
            jax.ShapeDtypeStruct(prev_values.shape, bf16),
            jax.ShapeDtypeStruct((heads, 2, props, seqs), f32),
        ),
        in_specs=[pl.BlockSpec(memory_space=pltpu.SMEM), anywhere] + [here] * 8,
        out_specs=[anywhere] + [here] * 5,
        scratch_shapes=[
            pltpu.VMEM((heads, seqs, size, size), f32),
            pltpu.SemaphoreType.DMA((heads,)),
            pltpu.SemaphoreType.DMA((heads,)),
        ],
        compiler_params=pltpu.CompilerParams(vmem_limit_bytes=58 * 1024 * 1024),
        cost_estimate=pl.CostEstimate(
            flops=2 * heads * seqs * size * size * 64, bytes_accessed=9 << 20, transcendentals=0
        ),
    )(accepted, state_c, state_n, inputs[12], prev_keys, prev_values, inputs[15], *fresh)
    return sent, new_c, new_n, new_m.T, keys, values, gates.transpose(3, 0, 1, 2)


def per_device(*arrays):
    inputs, out_weight = arrays[:9] + arrays[10:], arrays[9]
    parts = passed_on(out_weight)
    sent, *rest = cell(*inputs)
    mixed = project_out(sent, parts)
    return (mixed.reshape(-1, inputs[0].shape[1], mixed.shape[1]), *rest)


def solution(mesh):
    in_specs = (
        P("kv", None, None),
        P(),
        P(None, "tp"),
        P(None, "tp"),
        P(None, "tp"),
        P(None, "tp"),
        P(),
        P(),
        P("tp"),
        P("tp", "kv"),
        P("kv", "tp", None, None),
        P("kv", "tp", None),
        P("kv", "tp"),
        P("kv", "tp", None, None),
        P("kv", "tp", None, None),
        P("kv", "tp", None, None),
        P("kv"),
    )
    out_specs = (
        P(None, None, "kv"),
        P("kv", "tp", None, None),
        P("kv", "tp", None),
        P("kv", "tp"),
        P("kv", "tp", None, None),
        P("kv", "tp", None, None),
        P("kv", "tp", None, None),
    )
    return jax.shard_map(
        per_device, mesh=mesh, in_specs=in_specs, out_specs=out_specs, check_vma=False
    )
```

```python
import jax
import jax.numpy as jnp
from jax import lax
from jax.experimental import pallas as pl
from jax.experimental.pallas import tpu as pltpu
from jax.sharding import PartitionSpec as P


EPSILON = 1e-06
HIGHEST = lax.Precision.HIGHEST


def ring(count, step):
    return [(i, (i + step) % count) for i in range(count)]


def swap_cores(x):
    return lax.ppermute(x, "kv", [(i, i ^ 1) for i in range(lax.axis_size("kv"))])


def passed_on(weight):
    tp = lax.axis_size("tp")
    passed = [weight]
    for step in range(1, tp):
        passed.append(lax.ppermute(weight, "tp", ring(tp, step)))
    return passed


def mix_kernel(received, *refs):
    weights, out = refs[:-1], refs[-1]
    chips, tp, rows, depth = received.shape
    me = lax.axis_index("tp")
    core = lax.rem(lax.axis_index("kv"), 2)
    total = None
    for step in range(tp):
        source = lax.rem(me - step + tp, tp)
        part = received[:, pl.ds(source, 1)].reshape(chips * rows, depth)
        both = jnp.concatenate([weights[step][...], weights[tp + step][...]], axis=1)
        dot = jnp.dot(part, both, preferred_element_type=jnp.float32)
        total = dot if total is None else total + dot
    mixed = total.astype(jnp.bfloat16)
    columns = mixed.shape[1] // 2
    for x in range(tp):
        out[core, x] = mixed[:, :columns]
        out[1 - core, x] = mixed[:, columns:]


def same_core(kv, tp):
    return [
        [(chip * 2 + core) * tp + x for chip in range(kv // 2) for x in range(tp)]
        for core in (0, 1)
    ]


def same_line(kv, tp):
    return [
        [(chip * 2 + core) * tp + x for core in (0, 1) for x in range(tp)]
        for chip in range(kv // 2)
    ]


def project_out(sent, own_parts):
    kv, tp = lax.axis_size("kv"), lax.axis_size("tp")
    chips = kv // 2
    rows, depth = sent.shape[1] // tp, sent.shape[2]
    other_parts = [swap_cores(part) for part in own_parts]
    received = lax.all_to_all(
        sent.reshape(chips * tp, rows, depth), ("kv", "tp"), 0, 0,
        tiled=True, axis_index_groups=same_core(kv, tp),
    ).reshape(chips, tp, rows, depth)
    columns = own_parts[0].shape[1]
    mixed = pl.pallas_call(
        mix_kernel,
        out_shape=jax.ShapeDtypeStruct((2, tp, chips * rows, columns), jnp.bfloat16),
        compiler_params=pltpu.CompilerParams(vmem_limit_bytes=12 * 1024 * 1024),
        cost_estimate=pl.CostEstimate(
            flops=4 * chips * rows * tp * depth * columns,
            bytes_accessed=3 << 20,
            transcendentals=0,
        ),
    )(received, *own_parts, *other_parts)
    everyone = lax.all_to_all(
        mixed.reshape(2 * tp, chips * rows, columns), ("kv", "tp"), 0, 0,
        tiled=True, axis_index_groups=same_line(kv, tp),
    ).reshape(2, tp, chips, rows, columns)
    return everyone.transpose(2, 0, 1, 3, 4).reshape(-1, columns)


def split(x):
    high = x.astype(jnp.bfloat16)
    return high, (x - high.astype(jnp.float32)).astype(jnp.bfloat16)


def exact_dot(a, b, contract):
    return lax.dot_general(
        a, b, ((contract[:1], contract[1:]), ((), ())),
        precision=HIGHEST, preferred_element_type=jnp.float32,
    )


def dot_nt(a, b):
    return lax.dot_general(
        a, b, (((1,), (1,)), ((), ())), preferred_element_type=jnp.float32
    )


def log_sigmoid(x):
    return jnp.minimum(x, 0.0) - jnp.log1p(jnp.exp(-jnp.abs(x)))


def iota(shape, dim):
    return lax.broadcasted_iota(jnp.int32, shape, dim)


def bringer(sems):
    copies = []

    def bring(src, dst):
        copy = pltpu.make_async_copy(src, dst, sems.at[len(copies)])
        copies.append(copy)
        copy.start()
        return copy

    return bring


def arrive(some):
    for copy in some:
        copy.wait()


def spreads(seqs, rows):
    across = jnp.where(iota((seqs, rows), 0) == (iota((seqs, rows), 1) >> 2), 1.0, 0.0)
    down = jnp.where((iota((rows, seqs), 0) >> 2) == iota((rows, seqs), 1), 1.0, 0.0)
    return across, down


def replay(accepted, state_m, prev_gates, across):
    heads, _, props, seqs = prev_gates.shape
    seq_lane = iota((1, seqs), 1)
    counts = jnp.zeros((1, seqs), jnp.int32)
    for b in range(seqs):
        counts = jnp.where(seq_lane == b, accepted[b], counts)
    total = jnp.zeros((heads, seqs), jnp.float32)
    sums, inputs = [], []
    for s in range(props):
        both = [
            jnp.concatenate([prev_gates[h, g, s : s + 1, :] for h in range(heads)], axis=0)
            for g in (0, 1)
        ]
        total = total + jnp.where(counts > s, log_sigmoid(both[1]), 0.0)
        sums.append(total)
        inputs.append(both[0])
    logs = [
        jnp.where(counts > s, total - sums[s] + inputs[s], -jnp.inf) for s in range(props)
    ]
    decayed = total + state_m[...]
    stable = decayed
    for s in range(props):
        stable = jnp.maximum(stable, logs[s])
    shrink = jnp.exp(decayed - stable)
    prop_lane = iota((1, across.shape[1]), 1) & (props - 1)
    weights = jnp.zeros((heads, across.shape[1]), jnp.float32)
    for s in range(props):
        spaced = exact_dot(jnp.exp(logs[s] - stable), across, (1, 0))
        weights = weights + jnp.where(prop_lane == s, spaced, 0.0)
    return stable, shrink, weights


def cell_kernel(
    accepted,
    tokens,
    norm_gain,
    query_weight,
    key_weight,
    value_weight,
    outgate_weight,
    gate_weight,
    gate_bias,
    head_gain,
    state_c,
    state_n,
    state_m,
    prev_keys,
    prev_values,
    prev_gates,
    gated_out,
    keys_out,
    values_out,
    gates_out,
    accepted_s,
    tokens_v,
    gain_v,
    weights_v,
    gate_weight_v,
    gate_bias_v,
    head_gain_v,
    state_c_v,
    state_n_v,
    state_m_v,
    prev_keys_v,
    prev_values_v,
    prev_gates_v,
    normed_f,
    normed_v,
    recall_v,
    hidden_v,
    gated_v,
    keys_v,
    values_v,
    gates_v,
    sems,
    out_sems,
):
    f32, bf16 = jnp.float32, jnp.bfloat16
    seqs, props, width = tokens_v.shape
    heads, _, size, _ = state_c_v.shape
    rows = seqs * props
    heads_total = gate_weight_v.shape[0] // 2
    scale = size ** (-0.5)
    pieces = 4
    depth = width // pieces
    bring = bringer(sems)

    def bring_weight(which, src):
        return [
            bring(src.at[pl.ds(p * depth, depth)], weights_v.at[which, pl.ds(p * depth, depth)])
            for p in range(pieces)
        ]

    early = [bring(tokens, tokens_v), bring(norm_gain, gain_v)]
    gates_in = [bring(gate_weight, gate_weight_v), bring(gate_bias, gate_bias_v)]
    replay_in = [
        bring(accepted, accepted_s),
        bring(state_m, state_m_v),
        bring(prev_gates, prev_gates_v),
        bring(state_n, state_n_v),
        bring(prev_keys, prev_keys_v),
        bring(prev_values, prev_values_v),
        bring(head_gain, head_gain_v),
    ]
    weights_in = [bring_weight(0, query_weight)]
    states_in = [bring(state_c.at[:, h], state_c_v.at[h]) for h in range(heads)]
    weights_in += [
        bring_weight(1, key_weight),
        bring_weight(2, value_weight),
        bring_weight(3, outgate_weight),
    ]

    across, down = spreads(seqs, rows)
    square = (rows, rows)
    same = (iota(square, 0) >> 2) == (iota(square, 1) >> 2)
    causal = same & (iota(square, 0) >= iota(square, 1))

    arrive(early)
    gain = gain_v[...].astype(f32).reshape(1, width)
    for b in range(seqs):
        x = tokens_v[b].astype(f32)
        mean = jnp.mean(x * x, axis=-1, keepdims=True)
        normed_f[b * props : (b + 1) * props, :] = x * lax.rsqrt(mean + EPSILON) * gain
    normed_v[...] = normed_f[...].astype(bf16)

    arrive(gates_in)
    bias = jnp.concatenate([gate_bias_v[0:1, :], gate_bias_v[1:2, :]], axis=1)
    gates = dot_nt(normed_v[...], gate_weight_v[...]) + bias
    gates = jnp.concatenate([gates, jnp.zeros((rows, 128 - 2 * heads_total), f32)], axis=1)
    first_head = lax.axis_index("tp") * heads
    gates = pltpu.roll(gates, 128 - first_head, 1)
    cumul = exact_dot(jnp.where(causal, 1.0, 0.0), log_sigmoid(gates), (1, 0))
    gates_t = gates.T
    cumul_t = cumul.T
    gates_v[...] = gates_t[: 2 * heads_total]
    sends = [pltpu.make_async_copy(gates_v, gates_out, out_sems.at[0])]
    sends[0].start()

    arrive(replay_in)
    stable, shrink, weights = replay(accepted_s, state_m_v, prev_gates_v, across)
    weights = weights * scale
    stable_col = exact_dot(down, stable, (1, 1))
    shrink_col = exact_dot(down, shrink, (1, 1))

    def project(which):
        acc = None
        for p in range(pieces):
            weights_in[which][p].wait()
            part = jnp.dot(
                normed_v[:, p * depth : (p + 1) * depth],
                weights_v[which, p * depth : (p + 1) * depth, :],
                preferred_element_type=f32,
            )
            acc = part if acc is None else acc + part
        return acc.astype(bf16)

    queries = project(0)
    upper = iota((2 * props, size), 0) < props
    for h in range(heads):
        cols = slice(h * size, (h + 1) * size)
        query_f = queries[:, cols].astype(f32)
        states_in[h].wait()
        for p in range(seqs // 2):
            stacked = [
                state_c_v[h, b].astype(bf16) for b in (2 * p, 2 * p + 1)
            ]
            pair = slice(2 * p * props, 2 * (p + 1) * props)
            asked = query_f[pair].astype(bf16)
            found = dot_nt(asked, jnp.concatenate(stacked, axis=0))
            recall_v[pair, cols] = jnp.where(upper, found[:, :size], found[:, size:])

    new_keys = project(1)
    keys_v[...] = new_keys
    sends.append(pltpu.make_async_copy(keys_v, keys_out, out_sems.at[1]))
    sends[1].start()
    new_values = project(2)
    values_v[...] = new_values
    sends.append(pltpu.make_async_copy(values_v, values_out, out_sems.at[2]))
    sends[2].start()
    for h in range(heads):
        cols = slice(h * size, (h + 1) * size)
        query, key, value = queries[:, cols], new_keys[:, cols], new_values[:, cols]
        old_key = prev_keys_v[:, h].astype(f32).reshape(rows, size).astype(bf16)
        old_value = prev_values_v[:, h].astype(f32).reshape(rows, size).astype(bf16)
        c_col = cumul[:, heads_total + h : heads_total + h + 1]
        c_row = cumul_t[heads_total + h : heads_total + h + 1, :]
        i_row = gates_t[h : h + 1, :]
        logs_ts = jnp.where(causal, c_col - c_row + i_row, -jnp.inf)
        carried = c_col + stable_col[:, h : h + 1]
        steady = jnp.maximum(carried, jnp.max(logs_ts, axis=1, keepdims=True))
        weight_state = jnp.exp(carried - steady)
        scores = dot_nt(query, key) * scale * jnp.exp(logs_ts - steady)
        replayed = jnp.where(same, dot_nt(query, old_key) * weights[h : h + 1, :], 0.0)
        both = jnp.concatenate([weight_state * replayed, scores], axis=1)
        kept = weight_state * shrink_col[:, h : h + 1]
        numer = kept * recall_v[:, cols] + jnp.dot(
            jnp.concatenate(split(both), axis=1),
            jnp.concatenate([old_value, value] * 2, axis=0),
            preferred_element_type=f32,
        )
        along = exact_dot(query.astype(f32), state_n_v[:, h, :], (1, 1))
        recall_norm = jnp.sum(along * down, axis=1, keepdims=True)
        denom = kept * recall_norm + jnp.sum(both, axis=1, keepdims=True)
        hidden = numer / jnp.maximum(jnp.abs(denom), jnp.exp(-steady))
        hidden_v[:, cols] = hidden * lax.rsqrt(
            jnp.mean(hidden * hidden, axis=1, keepdims=True) + EPSILON
        )

    outgate = project(3)
    head_scale = head_gain_v[...].astype(f32).reshape(1, heads * size)
    gated_v[...] = (
        hidden_v[...] * head_scale * jax.nn.sigmoid(outgate.astype(f32))
    ).astype(bf16)
    for chip in range(gated_out.shape[0]):
        copy = pltpu.make_async_copy(gated_v, gated_out.at[chip], out_sems.at[3 + chip])
        copy.start()
        sends.append(copy)
    arrive(sends)


def keep_kernel(
    accepted,
    state_c,
    state_n,
    state_m,
    prev_keys,
    prev_values,
    prev_gates,
    new_keys,
    new_values,
    gates_t,
    carried_c,
    carried_n,
    carried_m,
    step_keys,
    step_values,
    step_gates,
    state_c_v,
    sems,
    out_sems,
):
    f32, bf16 = jnp.float32, jnp.bfloat16
    heads, seqs, size, _ = state_c_v.shape
    props = prev_gates.shape[2]
    rows = seqs * props
    scale = size ** (-0.5)
    bring = bringer(sems)
    states_in = [bring(state_c.at[:, h], state_c_v.at[h]) for h in range(heads)]
    across, _ = spreads(seqs, rows)
    for t in range(props):
        pick = jnp.where(iota((rows, seqs), 0) == iota((rows, seqs), 1) * props + t, 1.0, 0.0)
        picked = exact_dot(gates_t[...], pick, (1, 0))
        total = picked.shape[0] // 2
        for h in range(heads):
            step_gates[h, 0, t : t + 1, :] = picked[h : h + 1, :]
            step_gates[h, 1, t : t + 1, :] = picked[total + h : total + h + 1, :]
    stable, shrink, weights = replay(accepted, state_m, prev_gates, across)
    weights = weights * scale
    carried_m[...] = stable
    diagonal = jnp.where(iota((seqs, seqs), 0) == iota((seqs, seqs), 1), 1.0, 0.0)
    shrink_col = exact_dot(diagonal, shrink, (1, 1))
    seq_of_lane = (iota((1, 2 * rows), 1) & (rows - 1)) >> 2
    outs = []
    for h in range(heads):
        cols = slice(h * size, (h + 1) * size)
        step_keys[:, h] = new_keys[:, cols].astype(f32).reshape(seqs, props, size).astype(bf16)
        step_values[:, h] = new_values[:, cols].astype(f32).reshape(seqs, props, size).astype(bf16)
        keys = prev_keys[:, h].astype(f32).reshape(rows, size)
        values = prev_values[:, h].astype(f32).reshape(rows, size)
        weight = weights[h : h + 1, :]
        carried_n[:, h, :] = shrink_col[:, h : h + 1] * state_n[:, h, :] + exact_dot(
            across * weight, keys, (1, 0)
        )
        weighted = jnp.concatenate(split(values.T * weight), axis=1)
        key_pair = jnp.concatenate([keys, keys], axis=0).astype(bf16)
        states_in[h].wait()
        for b in range(seqs):
            mask = jnp.where(seq_of_lane == b, 1.0, 0.0).astype(bf16)
            update = jnp.dot(weighted * mask, key_pair, preferred_element_type=f32)
            state_c_v[h, b] = shrink[h : h + 1, b : b + 1] * state_c_v[h, b] + update
        copy = pltpu.make_async_copy(state_c_v.at[h], carried_c.at[:, h], out_sems.at[h])
        copy.start()
        outs.append(copy)
    arrive(outs)


def cell(
    tokens, norm_gain, query_weight, key_weight, value_weight, outgate_weight, gate_weight,
    gate_bias, head_gain, state_c, state_n, state_m, prev_keys, prev_values, prev_gates, accepted,
):
    f32, bf16 = jnp.float32, jnp.bfloat16
    seqs, props, width = tokens.shape
    heads, size = state_n.shape[1:]
    rows, columns = seqs * props, heads * size
    chips = lax.axis_size("kv") // 2
    inputs = (
        accepted,
        tokens,
        norm_gain,
        query_weight,
        key_weight,
        value_weight,
        outgate_weight,
        gate_weight.T,
        gate_bias,
        head_gain,
        state_c,
        state_n,
        state_m.T,
        prev_keys,
        prev_values,
        prev_gates.transpose(1, 2, 3, 0),
    )
    here = pl.BlockSpec(memory_space=pltpu.VMEM)
    anywhere = pl.BlockSpec(memory_space=pl.ANY)
    sent, *fresh = pl.pallas_call(
        cell_kernel,
        out_shape=(
            jax.ShapeDtypeStruct((chips, rows, columns), bf16),
            jax.ShapeDtypeStruct((rows, columns), bf16),
            jax.ShapeDtypeStruct((rows, columns), bf16),
            jax.ShapeDtypeStruct((gate_weight.shape[1], rows), f32),
        ),
        in_specs=[anywhere] * 16,
        out_specs=[anywhere] * 4,
        scratch_shapes=[
            pltpu.SMEM(accepted.shape, jnp.int32),
            pltpu.VMEM(tokens.shape, bf16),
            pltpu.VMEM((width,), bf16),
            pltpu.VMEM((4, width, columns), bf16),
            pltpu.VMEM(gate_weight.shape[::-1], bf16),
            pltpu.VMEM(gate_bias.shape, f32),
            pltpu.VMEM((columns,), bf16),
            pltpu.VMEM((heads, seqs, size, size), f32),
            pltpu.VMEM(state_n.shape, f32),
            pltpu.VMEM((heads, seqs), f32),
            pltpu.VMEM(prev_keys.shape, bf16),
            pltpu.VMEM(prev_values.shape, bf16),
            pltpu.VMEM((heads, 2, props, seqs), f32),
            pltpu.VMEM((rows, width), f32),
            pltpu.VMEM((rows, width), bf16),
            pltpu.VMEM((rows, columns), f32),
            pltpu.VMEM((rows, columns), f32),
            pltpu.VMEM((rows, columns), bf16),
            pltpu.VMEM((rows, columns), bf16),
            pltpu.VMEM((rows, columns), bf16),
            pltpu.VMEM((gate_weight.shape[1], rows), f32),
            pltpu.SemaphoreType.DMA((11 + 16 + heads,)),
            pltpu.SemaphoreType.DMA((3 + chips,)),
        ],
        compiler_params=pltpu.CompilerParams(vmem_limit_bytes=62 * 1024 * 1024),
        cost_estimate=pl.CostEstimate(
            flops=2 * rows * width * 4 * columns, bytes_accessed=22 << 20, transcendentals=0
        ),
    )(*inputs)
    new_c, new_n, new_m, keys, values, gates = pl.pallas_call(
        keep_kernel,
        out_shape=(
            jax.ShapeDtypeStruct(state_c.shape, f32),
            jax.ShapeDtypeStruct(state_n.shape, f32),
            jax.ShapeDtypeStruct((heads, seqs), f32),
            jax.ShapeDtypeStruct(prev_keys.shape, bf16),
            jax.ShapeDtypeStruct(prev_values.shape, bf16),
            jax.ShapeDtypeStruct((heads, 2, props, seqs), f32),
        ),
        in_specs=[pl.BlockSpec(memory_space=pltpu.SMEM), anywhere] + [here] * 8,
        out_specs=[anywhere] + [here] * 5,
        scratch_shapes=[
            pltpu.VMEM((heads, seqs, size, size), f32),
            pltpu.SemaphoreType.DMA((heads,)),
            pltpu.SemaphoreType.DMA((heads,)),
        ],
        compiler_params=pltpu.CompilerParams(vmem_limit_bytes=58 * 1024 * 1024),
        cost_estimate=pl.CostEstimate(
            flops=2 * heads * seqs * size * size * 64, bytes_accessed=9 << 20, transcendentals=0
        ),
    )(accepted, state_c, state_n, inputs[12], prev_keys, prev_values, inputs[15], *fresh)
    return sent, new_c, new_n, new_m.T, keys, values, gates.transpose(3, 0, 1, 2)


def per_device(*arrays):
    inputs, out_weight = arrays[:9] + arrays[10:], arrays[9]
    parts = passed_on(out_weight)
    sent, *rest = cell(*inputs)
    mixed = project_out(sent, parts)
    return (mixed.reshape(-1, inputs[0].shape[1], mixed.shape[1]), *rest)


def solution(mesh):
    in_specs = (
        P("kv", None, None),
        P(),
        P(None, "tp"),
        P(None, "tp"),
        P(None, "tp"),
        P(None, "tp"),
        P(),
        P(),
        P("tp"),
        P("tp", "kv"),
        P("kv", "tp", None, None),
        P("kv", "tp", None),
        P("kv", "tp"),
        P("kv", "tp", None, None),
        P("kv", "tp", None, None),
        P("kv", "tp", None, None),
        P("kv"),
    )
    out_specs = (
        P(None, None, "kv"),
        P("kv", "tp", None, None),
        P("kv", "tp", None),
        P("kv", "tp"),
        P("kv", "tp", None, None),
        P("kv", "tp", None, None),
        P("kv", "tp", None, None),
    )
    return jax.shard_map(
        per_device, mesh=mesh, in_specs=in_specs, out_specs=out_specs, check_vma=False
    )
```

```python
import jax
import jax.numpy as jnp
from jax import lax
from jax.experimental import pallas as pl
from jax.experimental.pallas import tpu as pltpu
from jax.sharding import PartitionSpec as P


EPSILON = 1e-06
HIGHEST = lax.Precision.HIGHEST


def ring(count, step):
    return [(i, (i + step) % count) for i in range(count)]


def swap_cores(x):
    return lax.ppermute(x, "kv", [(i, i ^ 1) for i in range(lax.axis_size("kv"))])


def passed_on(weight):
    tp = lax.axis_size("tp")
    passed = [weight]
    for step in range(1, tp):
        passed.append(lax.ppermute(weight, "tp", ring(tp, step)))
    return passed


def mix_kernel(received, *refs):
    weights, out = refs[:-1], refs[-1]
    chips, tp, rows, depth = received.shape
    me = lax.axis_index("tp")
    core = lax.rem(lax.axis_index("kv"), 2)
    total = None
    for step in range(tp):
        source = lax.rem(me - step + tp, tp)
        part = received[:, pl.ds(source, 1)].reshape(chips * rows, depth)
        both = jnp.concatenate([weights[step][...], weights[tp + step][...]], axis=1)
        dot = jnp.dot(part, both, preferred_element_type=jnp.float32)
        total = dot if total is None else total + dot
    mixed = total.astype(jnp.bfloat16)
    columns = mixed.shape[1] // 2
    for x in range(tp):
        out[core, x] = mixed[:, :columns]
        out[1 - core, x] = mixed[:, columns:]


def same_core(kv, tp):
    return [
        [(chip * 2 + core) * tp + x for chip in range(kv // 2) for x in range(tp)]
        for core in (0, 1)
    ]


def same_line(kv, tp):
    return [
        [(chip * 2 + core) * tp + x for core in (0, 1) for x in range(tp)]
        for chip in range(kv // 2)
    ]


def project_out(sent, own_parts):
    kv, tp = lax.axis_size("kv"), lax.axis_size("tp")
    chips = kv // 2
    rows, depth = sent.shape[1] // tp, sent.shape[2]
    other_parts = [swap_cores(part) for part in own_parts]
    received = lax.all_to_all(
        sent.reshape(chips * tp, rows, depth), ("kv", "tp"), 0, 0,
        tiled=True, axis_index_groups=same_core(kv, tp),
    ).reshape(chips, tp, rows, depth)
    columns = own_parts[0].shape[1]
    mixed = pl.pallas_call(
        mix_kernel,
        out_shape=jax.ShapeDtypeStruct((2, tp, chips * rows, columns), jnp.bfloat16),
        compiler_params=pltpu.CompilerParams(vmem_limit_bytes=12 * 1024 * 1024),
        cost_estimate=pl.CostEstimate(
            flops=4 * chips * rows * tp * depth * columns,
            bytes_accessed=3 << 20,
            transcendentals=0,
        ),
    )(received, *own_parts, *other_parts)
    everyone = lax.all_to_all(
        mixed.reshape(2 * tp, chips * rows, columns), ("kv", "tp"), 0, 0,
        tiled=True, axis_index_groups=same_line(kv, tp),
    ).reshape(2, tp, chips, rows, columns)
    return everyone.transpose(2, 0, 1, 3, 4).reshape(-1, columns)


def split(x):
    high = x.astype(jnp.bfloat16)
    return high, (x - high.astype(jnp.float32)).astype(jnp.bfloat16)


def exact_dot(a, b, contract):
    return lax.dot_general(
        a, b, ((contract[:1], contract[1:]), ((), ())),
        precision=HIGHEST, preferred_element_type=jnp.float32,
    )


def dot_nt(a, b):
    return lax.dot_general(
        a, b, (((1,), (1,)), ((), ())), preferred_element_type=jnp.float32
    )


def log_sigmoid(x):
    return jnp.minimum(x, 0.0) - jnp.log1p(jnp.exp(-jnp.abs(x)))


def iota(shape, dim):
    return lax.broadcasted_iota(jnp.int32, shape, dim)


def bringer(sems):
    copies = []

    def bring(src, dst):
        copy = pltpu.make_async_copy(src, dst, sems.at[len(copies)])
        copies.append(copy)
        copy.start()
        return copy

    return bring


def arrive(some):
    for copy in some:
        copy.wait()


def spreads(seqs, rows):
    across = jnp.where(iota((seqs, rows), 0) == (iota((seqs, rows), 1) >> 2), 1.0, 0.0)
    down = jnp.where((iota((rows, seqs), 0) >> 2) == iota((rows, seqs), 1), 1.0, 0.0)
    return across, down


def replay(accepted, state_m, prev_gates, across):
    heads, _, props, seqs = prev_gates.shape
    seq_lane = iota((1, seqs), 1)
    counts = jnp.zeros((1, seqs), jnp.int32)
    for b in range(seqs):
        counts = jnp.where(seq_lane == b, accepted[b], counts)
    total = jnp.zeros((heads, seqs), jnp.float32)
    sums, inputs = [], []
    for s in range(props):
        both = [
            jnp.concatenate([prev_gates[h, g, s : s + 1, :] for h in range(heads)], axis=0)
            for g in (0, 1)
        ]
        total = total + jnp.where(counts > s, log_sigmoid(both[1]), 0.0)
        sums.append(total)
        inputs.append(both[0])
    logs = [
        jnp.where(counts > s, total - sums[s] + inputs[s], -jnp.inf) for s in range(props)
    ]
    decayed = total + state_m[...]
    stable = decayed
    for s in range(props):
        stable = jnp.maximum(stable, logs[s])
    shrink = jnp.exp(decayed - stable)
    prop_lane = iota((1, across.shape[1]), 1) & (props - 1)
    weights = jnp.zeros((heads, across.shape[1]), jnp.float32)
    for s in range(props):
        spaced = exact_dot(jnp.exp(logs[s] - stable), across, (1, 0))
        weights = weights + jnp.where(prop_lane == s, spaced, 0.0)
    return stable, shrink, weights


def cell_kernel(
    accepted,
    tokens,
    norm_gain,
    query_weight,
    key_weight,
    value_weight,
    outgate_weight,
    gate_weight,
    gate_bias,
    head_gain,
    state_c,
    state_n,
    state_m,
    prev_keys,
    prev_values,
    prev_gates,
    gated_out,
    keys_out,
    values_out,
    gates_out,
    accepted_s,
    tokens_v,
    gain_v,
    weights_v,
    gate_weight_v,
    gate_bias_v,
    head_gain_v,
    state_c_v,
    state_n_v,
    state_m_v,
    prev_keys_v,
    prev_values_v,
    prev_gates_v,
    normed_f,
    normed_v,
    recall_v,
    hidden_v,
    gated_v,
    keys_v,
    values_v,
    gates_v,
    decay_v,
    replayed_v,
    both_v,
    sems,
    out_sems,
):
    f32, bf16 = jnp.float32, jnp.bfloat16
    seqs, props, width = tokens_v.shape
    heads, _, size, _ = state_c_v.shape
    rows = seqs * props
    heads_total = gate_weight_v.shape[0] // 2
    scale = size ** (-0.5)
    pieces = 4
    depth = width // pieces
    bring = bringer(sems)

    def bring_weight(which, src):
        return [
            bring(src.at[pl.ds(p * depth, depth)], weights_v.at[which, pl.ds(p * depth, depth)])
            for p in range(pieces)
        ]

    early = [bring(tokens, tokens_v), bring(norm_gain, gain_v)]
    gates_in = [bring(gate_weight, gate_weight_v), bring(gate_bias, gate_bias_v)]
    replay_in = [
        bring(accepted, accepted_s),
        bring(state_m, state_m_v),
        bring(prev_gates, prev_gates_v),
        bring(state_n, state_n_v),
        bring(prev_keys, prev_keys_v),
        bring(prev_values, prev_values_v),
        bring(head_gain, head_gain_v),
    ]
    weights_in = [bring_weight(0, query_weight)]
    states_in = [bring(state_c.at[:, h], state_c_v.at[h]) for h in range(heads)]
    weights_in += [
        bring_weight(1, key_weight),
        bring_weight(2, value_weight),
        bring_weight(3, outgate_weight),
    ]

    across, down = spreads(seqs, rows)
    square = (rows, rows)
    same = (iota(square, 0) >> 2) == (iota(square, 1) >> 2)
    causal = same & (iota(square, 0) >= iota(square, 1))

    arrive(early)
    gain = gain_v[...].astype(f32).reshape(1, width)
    for b in range(seqs):
        x = tokens_v[b].astype(f32)
        mean = jnp.mean(x * x, axis=-1, keepdims=True)
        normed_f[b * props : (b + 1) * props, :] = x * lax.rsqrt(mean + EPSILON) * gain
    normed_v[...] = normed_f[...].astype(bf16)

    arrive(gates_in)
    bias = jnp.concatenate([gate_bias_v[0:1, :], gate_bias_v[1:2, :]], axis=1)
    gates = dot_nt(normed_v[...], gate_weight_v[...]) + bias
    gates = jnp.concatenate([gates, jnp.zeros((rows, 128 - 2 * heads_total), f32)], axis=1)
    first_head = lax.axis_index("tp") * heads
    gates = pltpu.roll(gates, 128 - first_head, 1)
    cumul = exact_dot(jnp.where(causal, 1.0, 0.0), log_sigmoid(gates), (1, 0))
    gates_t = gates.T
    cumul_t = cumul.T
    gates_v[...] = gates_t[: 2 * heads_total]
    sends = [pltpu.make_async_copy(gates_v, gates_out, out_sems.at[0])]
    sends[0].start()

    arrive(replay_in)
    stable, shrink, weights = replay(accepted_s, state_m_v, prev_gates_v, across)
    weights = weights * scale
    stable_col = exact_dot(down, stable, (1, 1))
    shrink_col = exact_dot(down, shrink, (1, 1))

    def project(which):
        acc = None
        for p in range(pieces):
            weights_in[which][p].wait()
            part = jnp.dot(
                normed_v[:, p * depth : (p + 1) * depth],
                weights_v[which, p * depth : (p + 1) * depth, :],
                preferred_element_type=f32,
            )
            acc = part if acc is None else acc + part
        return acc

    queries = project(0).astype(bf16)

    def before(h):
        cols = slice(h * size, (h + 1) * size)
        query = queries[:, cols]
        old_key = prev_keys_v[:, h].astype(f32).reshape(rows, size).astype(bf16)
        c_col = cumul[:, heads_total + h : heads_total + h + 1]
        c_row = cumul_t[heads_total + h : heads_total + h + 1, :]
        i_row = gates_t[h : h + 1, :]
        logs_ts = jnp.where(causal, c_col - c_row + i_row, -jnp.inf)
        carried = c_col + stable_col[:, h : h + 1]
        steady = jnp.maximum(carried, jnp.max(logs_ts, axis=1, keepdims=True))
        weight_state = jnp.exp(carried - steady)
        decay_v[h] = scale * jnp.exp(logs_ts - steady)
        replayed = jnp.where(same, dot_nt(query, old_key) * weights[h : h + 1, :], 0.0)
        replayed = weight_state * replayed
        replayed_v[h] = replayed
        kept = weight_state * shrink_col[:, h : h + 1]
        along = exact_dot(query.astype(f32), state_n_v[:, h, :], (1, 1))
        denom = kept * jnp.sum(along * down, axis=1, keepdims=True)
        denom = denom + jnp.sum(replayed, axis=1, keepdims=True)
        return kept, denom, jnp.exp(-steady)

    upper = iota((2 * props, size), 0) < props
    starts = []
    firsts = [before(h) for h in range(heads)]
    for h in range(heads):
        cols = slice(h * size, (h + 1) * size)
        query_f = queries[:, cols].astype(f32)
        kept, denom, least = firsts[h]
        starts.append((denom, least))
        states_in[h].wait()
        for p in range(seqs // 2):
            stacked = [
                state_c_v[h, b].astype(bf16) for b in (2 * p, 2 * p + 1)
            ]
            pair = slice(2 * p * props, 2 * (p + 1) * props)
            asked = query_f[pair].astype(bf16)
            found = dot_nt(asked, jnp.concatenate(stacked, axis=0))
            recall_v[pair, cols] = jnp.where(upper, found[:, :size], found[:, size:])
        recall_v[:, cols] = kept * recall_v[:, cols]

    new_keys = project(1).astype(bf16)
    keys_v[...] = new_keys
    sends.append(pltpu.make_async_copy(keys_v, keys_out, out_sems.at[1]))
    sends[1].start()
    ready = []
    for h in range(heads):
        cols = slice(h * size, (h + 1) * size)
        scores = dot_nt(queries[:, cols], new_keys[:, cols]) * decay_v[h]
        denom, least = starts[h]
        denom = denom + jnp.sum(scores, axis=1, keepdims=True)
        ready.append(1.0 / jnp.maximum(jnp.abs(denom), least))
        both_v[h] = jnp.concatenate(
            split(jnp.concatenate([replayed_v[h], scores], axis=1)), axis=1
        )
    new_values = project(2).astype(bf16)
    values_v[...] = new_values
    sends.append(pltpu.make_async_copy(values_v, values_out, out_sems.at[2]))
    sends[2].start()
    for h in range(heads):
        cols = slice(h * size, (h + 1) * size)
        old_value = prev_values_v[:, h].astype(f32).reshape(rows, size).astype(bf16)
        numer = recall_v[:, cols] + jnp.dot(
            both_v[h],
            jnp.concatenate([old_value, new_values[:, cols]] * 2, axis=0),
            preferred_element_type=f32,
        )
        hidden = numer * ready[h]
        hidden_v[:, cols] = hidden * lax.rsqrt(
            jnp.mean(hidden * hidden, axis=1, keepdims=True) + EPSILON
        )

    outgate = project(3).astype(bf16)
    head_scale = head_gain_v[...].astype(f32).reshape(1, heads * size)
    gated_v[...] = (
        hidden_v[...] * head_scale * jax.nn.sigmoid(outgate.astype(f32))
    ).astype(bf16)
    for chip in range(gated_out.shape[0]):
        copy = pltpu.make_async_copy(gated_v, gated_out.at[chip], out_sems.at[3 + chip])
        copy.start()
        sends.append(copy)
    arrive(sends)


def keep_kernel(
    accepted,
    state_c,
    state_n,
    state_m,
    prev_keys,
    prev_values,
    prev_gates,
    new_keys,
    new_values,
    gates_t,
    carried_c,
    carried_n,
    carried_m,
    step_keys,
    step_values,
    step_gates,
    state_c_v,
    sems,
    out_sems,
):
    f32, bf16 = jnp.float32, jnp.bfloat16
    heads, seqs, size, _ = state_c_v.shape
    props = prev_gates.shape[2]
    rows = seqs * props
    scale = size ** (-0.5)
    bring = bringer(sems)
    states_in = [bring(state_c.at[:, h], state_c_v.at[h]) for h in range(heads)]
    across, _ = spreads(seqs, rows)
    for t in range(props):
        pick = jnp.where(iota((rows, seqs), 0) == iota((rows, seqs), 1) * props + t, 1.0, 0.0)
        picked = exact_dot(gates_t[...], pick, (1, 0))
        total = picked.shape[0] // 2
        for h in range(heads):
            step_gates[h, 0, t : t + 1, :] = picked[h : h + 1, :]
            step_gates[h, 1, t : t + 1, :] = picked[total + h : total + h + 1, :]
    stable, shrink, weights = replay(accepted, state_m, prev_gates, across)
    weights = weights * scale
    carried_m[...] = stable
    diagonal = jnp.where(iota((seqs, seqs), 0) == iota((seqs, seqs), 1), 1.0, 0.0)
    shrink_col = exact_dot(diagonal, shrink, (1, 1))
    seq_of_lane = (iota((1, 2 * rows), 1) & (rows - 1)) >> 2
    outs = []
    for h in range(heads):
        cols = slice(h * size, (h + 1) * size)
        step_keys[:, h] = new_keys[:, cols].astype(f32).reshape(seqs, props, size).astype(bf16)
        step_values[:, h] = new_values[:, cols].astype(f32).reshape(seqs, props, size).astype(bf16)
        keys = prev_keys[:, h].astype(f32).reshape(rows, size)
        values = prev_values[:, h].astype(f32).reshape(rows, size)
        weight = weights[h : h + 1, :]
        carried_n[:, h, :] = shrink_col[:, h : h + 1] * state_n[:, h, :] + exact_dot(
            across * weight, keys, (1, 0)
        )
        weighted = jnp.concatenate(split(values.T * weight), axis=1)
        key_pair = jnp.concatenate([keys, keys], axis=0).astype(bf16)
        states_in[h].wait()
        for b in range(seqs):
            mask = jnp.where(seq_of_lane == b, 1.0, 0.0).astype(bf16)
            update = jnp.dot(weighted * mask, key_pair, preferred_element_type=f32)
            state_c_v[h, b] = shrink[h : h + 1, b : b + 1] * state_c_v[h, b] + update
        copy = pltpu.make_async_copy(state_c_v.at[h], carried_c.at[:, h], out_sems.at[h])
        copy.start()
        outs.append(copy)
    arrive(outs)


def cell(
    tokens, norm_gain, query_weight, key_weight, value_weight, outgate_weight, gate_weight,
    gate_bias, head_gain, state_c, state_n, state_m, prev_keys, prev_values, prev_gates, accepted,
):
    f32, bf16 = jnp.float32, jnp.bfloat16
    seqs, props, width = tokens.shape
    heads, size = state_n.shape[1:]
    rows, columns = seqs * props, heads * size
    chips = lax.axis_size("kv") // 2
    inputs = (
        accepted,
        tokens,
        norm_gain,
        query_weight,
        key_weight,
        value_weight,
        outgate_weight,
        gate_weight.T,
        gate_bias,
        head_gain,
        state_c,
        state_n,
        state_m.T,
        prev_keys,
        prev_values,
        prev_gates.transpose(1, 2, 3, 0),
    )
    here = pl.BlockSpec(memory_space=pltpu.VMEM)
    anywhere = pl.BlockSpec(memory_space=pl.ANY)
    sent, *fresh = pl.pallas_call(
        cell_kernel,
        out_shape=(
            jax.ShapeDtypeStruct((chips, rows, columns), bf16),
            jax.ShapeDtypeStruct((rows, columns), bf16),
            jax.ShapeDtypeStruct((rows, columns), bf16),
            jax.ShapeDtypeStruct((gate_weight.shape[1], rows), f32),
        ),
        in_specs=[anywhere] * 16,
        out_specs=[anywhere] * 4,
        scratch_shapes=[
            pltpu.SMEM(accepted.shape, jnp.int32),
            pltpu.VMEM(tokens.shape, bf16),
            pltpu.VMEM((width,), bf16),
            pltpu.VMEM((4, width, columns), bf16),
            pltpu.VMEM(gate_weight.shape[::-1], bf16),
            pltpu.VMEM(gate_bias.shape, f32),
            pltpu.VMEM((columns,), bf16),
            pltpu.VMEM((heads, seqs, size, size), f32),
            pltpu.VMEM(state_n.shape, f32),
            pltpu.VMEM((heads, seqs), f32),
            pltpu.VMEM(prev_keys.shape, bf16),
            pltpu.VMEM(prev_values.shape, bf16),
            pltpu.VMEM((heads, 2, props, seqs), f32),
            pltpu.VMEM((rows, width), f32),
            pltpu.VMEM((rows, width), bf16),
            pltpu.VMEM((rows, columns), f32),
            pltpu.VMEM((rows, columns), f32),
            pltpu.VMEM((rows, columns), bf16),
            pltpu.VMEM((rows, columns), bf16),
            pltpu.VMEM((rows, columns), bf16),
            pltpu.VMEM((gate_weight.shape[1], rows), f32),
            pltpu.VMEM((heads, rows, rows), f32),
            pltpu.VMEM((heads, rows, rows), f32),
            pltpu.VMEM((heads, rows, 4 * rows), bf16),
            pltpu.SemaphoreType.DMA((11 + 16 + heads,)),
            pltpu.SemaphoreType.DMA((3 + chips,)),
        ],
        compiler_params=pltpu.CompilerParams(vmem_limit_bytes=62 * 1024 * 1024),
        cost_estimate=pl.CostEstimate(
            flops=2 * rows * width * 4 * columns, bytes_accessed=22 << 20, transcendentals=0
        ),
    )(*inputs)
    new_c, new_n, new_m, keys, values, gates = pl.pallas_call(
        keep_kernel,
        out_shape=(
            jax.ShapeDtypeStruct(state_c.shape, f32),
            jax.ShapeDtypeStruct(state_n.shape, f32),
            jax.ShapeDtypeStruct((heads, seqs), f32),
            jax.ShapeDtypeStruct(prev_keys.shape, bf16),
            jax.ShapeDtypeStruct(prev_values.shape, bf16),
            jax.ShapeDtypeStruct((heads, 2, props, seqs), f32),
        ),
        in_specs=[pl.BlockSpec(memory_space=pltpu.SMEM), anywhere] + [here] * 8,
        out_specs=[anywhere] + [here] * 5,
        scratch_shapes=[
            pltpu.VMEM((heads, seqs, size, size), f32),
            pltpu.SemaphoreType.DMA((heads,)),
            pltpu.SemaphoreType.DMA((heads,)),
        ],
        compiler_params=pltpu.CompilerParams(vmem_limit_bytes=58 * 1024 * 1024),
        cost_estimate=pl.CostEstimate(
            flops=2 * heads * seqs * size * size * 64, bytes_accessed=9 << 20, transcendentals=0
        ),
    )(accepted, state_c, state_n, inputs[12], prev_keys, prev_values, inputs[15], *fresh)
    return sent, new_c, new_n, new_m.T, keys, values, gates.transpose(3, 0, 1, 2)


def per_device(*arrays):
    inputs, out_weight = arrays[:9] + arrays[10:], arrays[9]
    parts = passed_on(out_weight)
    sent, *rest = cell(*inputs)
    mixed = project_out(sent, parts)
    return (mixed.reshape(-1, inputs[0].shape[1], mixed.shape[1]), *rest)


def solution(mesh):
    in_specs = (
        P("kv", None, None),
        P(),
        P(None, "tp"),
        P(None, "tp"),
        P(None, "tp"),
        P(None, "tp"),
        P(),
        P(),
        P("tp"),
        P("tp", "kv"),
        P("kv", "tp", None, None),
        P("kv", "tp", None),
        P("kv", "tp"),
        P("kv", "tp", None, None),
        P("kv", "tp", None, None),
        P("kv", "tp", None, None),
        P("kv"),
    )
    out_specs = (
        P(None, None, "kv"),
        P("kv", "tp", None, None),
        P("kv", "tp", None),
        P("kv", "tp"),
        P("kv", "tp", None, None),
        P("kv", "tp", None, None),
        P("kv", "tp", None, None),
    )
    return jax.shard_map(
        per_device, mesh=mesh, in_specs=in_specs, out_specs=out_specs, check_vma=False
    )
```
